32 devices in a mesh: ep: 8 (over z, x), tp: 4 (over y, core).
Axes of the slice: x: 2, y: 2, z: 4, core: 2. Of those that a mesh axis runs over, the one named last changes fastest.
Arguments:
- query_rows: bfloat16 [3072, 4096], P('ep', 'tp'), may hold values from -6 to 6
- key_rows: bfloat16 [3072, 2048], P('ep', 'tp'), may hold values from -6 to 6
- value_rows: bfloat16 [3072, 2048], P('ep', 'tp'), may hold values from -6 to 6
- query_gain: float32 [128], replicated, may hold values from 0.4 to 5
- key_gain: float32 [128], replicated, may hold values from 0.4 to 5
- w_out: bfloat16 [4096, 2048], P('tp'), may hold values from -0.09375 to 0.09375
- mixer_gain: float32 [2048], replicated, may hold values from 0.1 to 1.9
- expert_input: bfloat16 [1536, 2048], P('ep'), may hold values from -6 to 6
- expert_ids: int32 [1536, 2], P('ep'), may hold values from 0 to 7, as said below
- expert_weights: float32 [1536, 2], P('ep'), may hold values from 0.1 to 1
- input_gain: float32 [2048], replicated, may hold values from 0.1 to 1.9
- w_gate: bfloat16 [8, 2048, 4096], P('ep', None, 'tp'), may hold values from -0.125 to 0.125
- w_up: bfloat16 [8, 2048, 4096], P('ep', None, 'tp'), may hold values from -0.125 to 0.125
- w_down: bfloat16 [8, 4096, 2048], P('ep', 'tp'), may hold values from -2 to 2
- out_gain: float32 [2048], P('tp'), may hold values from 0.1 to 1.9
Outputs:
- mixer_result: bfloat16 [3072, 2048], P(('ep', 'tp'))
- moe_result: bfloat16 [1536, 2048], P('ep', 'tp')
The draws below stay inside these ranges and needn't reach their ends.
Inputs may be any that keep to these rules, and one draw needn't show every extreme that they name: `expert_ids`: the two experts of a row differ and lie in one group of 2 consecutive experts. Among the rows of one index of ep (aligned blocks of 192 rows) no expert is named by more than 72 rows, and in every block some expert is named by exactly 72 rows.
All inputs are finite; a program needn't handle non-finite values.
Results may differ from the reference program's by a relative error of at most 0.02.
The reference program's roundings to bfloat16 on the way count: a program that leaves them out, or rounds other values in their place, can miss the bound.
Values may be sent and summed in bfloat16 or wider, within the bound.
A program may use at most 64 MiB of HBM per device.

```python
import math
import jax
import jax.numpy as jnp
from jax import lax

D = 2048
HEADS = 32
KV_HEADS = 16
HEAD = 128
GRID = 64
FF = 4096
GROUPS = 4
TOP = 2
ROWS2 = 192
EXPERTS = 8
INNER = 2
CAP = 72
TOK1 = 3072
TOK2 = 1536
N_EP = 8
N_TP = 4


def key_field(key):
    normal_base = jax.random.normal(jax.random.fold_in(key, 11), (TOK1, KV_HEADS * HEAD), jnp.float32)
    return jnp.clip(normal_base, -6.0, 6.0)


def draw_key_rows(key, part):
    return key_field(key).astype(jnp.bfloat16)


def draw_query_rows(key, part):
    fresh = jax.random.normal(jax.random.fold_in(key, 12), (TOK1, HEADS * HEAD), jnp.float32)
    return jnp.clip(fresh, -6.0, 6.0).astype(jnp.bfloat16)


def gain_field(key, offset):
    return jax.random.uniform(jax.random.fold_in(key, offset), (HEAD,), jnp.float32, 0.4, 1.6)


def draw_query_gain(key, part):
    return gain_field(key, 31)


def draw_key_gain(key, part):
    return gain_field(key, 32)


def draw_w_down(key, part):
    normal_base = jax.random.normal(jax.random.fold_in(key, 21), (EXPERTS, FF, D), jnp.float32) * FF ** (-0.5)
    column_ramp = jnp.exp(2.3 * jnp.arange(D, dtype=jnp.float32) / D)
    jitter = jax.random.uniform(jax.random.fold_in(key, 22), (D,), jnp.float32, 0.5, 1.5)
    return jnp.clip(normal_base * column_ramp * jitter, -2.0, 2.0).astype(jnp.bfloat16)


def block_ids(block_key):
    eighth = ROWS2 // 8
    shares = jnp.array([1, 2, 2, 3], jnp.int32)[jax.random.permutation(jax.random.fold_in(block_key, 1), 4)]
    group_sizes = shares * eighth
    group_ends = jnp.cumsum(group_sizes)
    starts = group_ends - group_sizes
    row_order = jnp.arange(ROWS2, dtype=jnp.int32)
    group_of = jnp.sum((row_order[:, None] >= group_ends[None, :]).astype(jnp.int32), axis=1)
    within = row_order - starts[group_of]
    shifts = jax.random.randint(jax.random.fold_in(block_key, 2), (GROUPS,), 1, INNER)
    labels = jax.vmap(lambda offset: jax.random.permutation(jax.random.fold_in(block_key, offset), INNER))(jnp.arange(GROUPS) + 3)
    first_pick = labels[group_of, within % INNER]
    second_pick = labels[group_of, (within + shifts[group_of]) % INNER]
    chosen_ids = jnp.stack([first_pick, second_pick], axis=1) + INNER * group_of[:, None]
    shuffle = jax.random.permutation(jax.random.fold_in(block_key, 9), ROWS2)
    return chosen_ids[shuffle].astype(jnp.int32)


def draw_expert_ids(key, part):
    block_keys = jax.vmap(lambda block_index: jax.random.fold_in(key, block_index))(jnp.arange(N_EP) + 100)
    return jax.vmap(block_ids)(block_keys).reshape(TOK2, TOP)


def shard_levels(own_key, dims, shards, smallest, top_value):
    loudness, own = 1.0, jax.random.fold_in(own_key, 6)
    for dim, parts in shards:
        steps = jnp.exp(jax.random.uniform(jax.random.fold_in(own, dim), (parts,), jnp.float32, smallest / len(shards), top_value / len(shards)))
        loudness = loudness * jnp.repeat(steps, dims[dim] // parts).reshape([-1 if axis == dim else 1 for axis in range(len(dims))])
    return loudness


def scatter_about(rng, dims, width, reach, pieces=(), held_as=jnp.bfloat16):
    level = shard_levels(rng, dims, pieces, -0.22, 0.18) if pieces else 1.0
    drawn = jax.random.normal(rng, dims, jnp.float32) * width * level
    return jnp.minimum(jnp.maximum(drawn, -reach), reach).astype(held_as)


def setup_inputs(seed: int = 0) -> dict:
    key_list = jax.random.split(jax.random.key(seed), 16)
    query_rows = draw_query_rows(jax.random.fold_in(key_list[15], 71), 0)
    key_rows = draw_key_rows(jax.random.fold_in(key_list[15], 71), 0)
    value_rows = scatter_about(key_list[2], (TOK1, KV_HEADS * HEAD), 1.0, 6.0, ((0, 8), (1, 4)))
    query_gain = draw_query_gain(jax.random.fold_in(key_list[15], 71), 0)
    key_gain = draw_key_gain(jax.random.fold_in(key_list[15], 71), 0)
    w_out = scatter_about(key_list[5], (HEADS * HEAD, D), (HEADS * HEAD) ** -0.5, 0.09375, ((0, 4),))
    mixer_gain = jnp.clip(1.0 + 0.18 * jax.random.normal(key_list[6], (D,), jnp.float32), 0.1, 1.9)
    expert_input = scatter_about(key_list[7], (TOK2, D), 1.0, 6.0, ((0, 8),))
    expert_ids = draw_expert_ids(jax.random.fold_in(key_list[15], 71), 0)
    expert_weights = jnp.clip(jnp.exp(math.log(1.0) - 2.3025851 * jax.random.uniform(key_list[9], (TOK2, TOP), jnp.float32) ** shard_levels(key_list[9], (TOK2, TOP), ((0, 8),), -0.2, 0.2)), 0.1, 1.0)
    input_gain = jnp.clip(1.0 + 0.18 * jax.random.normal(key_list[10], (D,), jnp.float32), 0.1, 1.9)
    w_gate = scatter_about(key_list[11], (EXPERTS, D, FF), D ** -0.5, 0.125, ((0, 8), (2, 4)))
    w_up = scatter_about(key_list[12], (EXPERTS, D, FF), D ** -0.5, 0.125, ((0, 8), (2, 4)))
    w_down = draw_w_down(jax.random.fold_in(key_list[15], 71), 0)
    out_gain = jnp.clip(1.0 + 0.18 * jax.random.normal(key_list[14], (D,), jnp.float32), 0.1, 1.9)
    return {"query_rows": query_rows, "key_rows": key_rows, "value_rows": value_rows, "query_gain": query_gain, "key_gain": key_gain, "w_out": w_out, "mixer_gain": mixer_gain, "expert_input": expert_input, "expert_ids": expert_ids, "expert_weights": expert_weights, "input_gain": input_gain, "w_gate": w_gate, "w_up": w_up, "w_down": w_down, "out_gain": out_gain}


EPS = 1e-06
THETA = 10000.0

def turn_half(half_part, position):
    half_width = half_part.shape[-1]
    frequency = THETA ** (-jnp.arange(0, half_width, 2, dtype=jnp.float32) / half_width)
    angles = position[:, None, None] * frequency[None, None, :]
    cosine = jnp.cos(angles)
    sine_part = jnp.sin(angles)
    first_half = half_part[..., :half_width // 2]
    second = half_part[..., half_width // 2:]
    return jnp.concatenate([first_half * cosine - second * sine_part, second * cosine + first_half * sine_part], axis=-1)

def norm_turn(raw_rows, gain_vec, row_offset):
    row_count = raw_rows.shape[0]
    head_dim = gain_vec.shape[0]
    head_count = raw_rows.shape[1] // head_dim
    by_head = raw_rows.astype(jnp.float32).reshape(row_count, head_count, head_dim)
    scaled = by_head * lax.rsqrt(lax.optimization_barrier(jnp.mean(by_head * by_head, axis=-1, keepdims=True)) + EPS) * gain_vec
    position = row_offset + jnp.arange(row_count, dtype=jnp.int32)
    grid_row = (position // GRID).astype(jnp.float32)
    grid_col = (position % GRID).astype(jnp.float32)
    half_dim = head_dim // 2
    turned = jnp.concatenate([turn_half(scaled[..., :half_dim], grid_row), turn_half(scaled[..., half_dim:], grid_col)], axis=-1)
    return turned.reshape(row_count, head_count * head_dim).astype(jnp.bfloat16)

def mixer_ref(query_rows, key_rows, value_rows, query_gain, key_gain, w_out, mixer_gain):
    token_count = query_rows.shape[0]
    group_size = HEADS // KV_HEADS
    query_turned = norm_turn(query_rows, query_gain, 0)
    key_turned = norm_turn(key_rows, key_gain, 0)
    query_heads = query_turned.reshape(token_count, HEADS, HEAD).transpose(1, 0, 2)
    key_heads = jnp.repeat(key_turned.reshape(token_count, KV_HEADS, HEAD).transpose(1, 0, 2), group_size, axis=0)
    value_heads = jnp.repeat(value_rows.reshape(token_count, KV_HEADS, HEAD).transpose(1, 0, 2), group_size, axis=0)

    def one_head(head_triple):
        query_head, key_head, value_head = head_triple
        scores = jnp.dot(query_head, key_head.T, preferred_element_type=jnp.float32) * HEAD ** (-0.5)
        row_max = lax.optimization_barrier(jnp.max(scores, axis=1, keepdims=True))
        exponent = jnp.exp(scores - row_max)
        probs = exponent.astype(jnp.bfloat16)
        numer = jnp.dot(probs, value_head, preferred_element_type=jnp.float32)
        return (numer / lax.optimization_barrier(jnp.sum(exponent, axis=1, keepdims=True))).astype(jnp.bfloat16)
    attended = lax.map(one_head, (query_heads, key_heads, value_heads))
    attended = attended.transpose(1, 0, 2).reshape(token_count, HEADS * HEAD)
    block_width = HEADS * HEAD // N_TP
    attended_blocks = attended.reshape(token_count, N_TP, block_width).transpose(1, 0, 2)
    weight_blocks = w_out.reshape(N_TP, block_width, D)

    def add_part(running_sum, block_pair):
        attended_block, weight_block = block_pair
        head_part = jnp.dot(attended_block, weight_block, preferred_element_type=jnp.float32).astype(jnp.bfloat16)
        head_part = lax.optimization_barrier(head_part)
        return (running_sum + head_part.astype(jnp.float32), None)
    mixed_sum, _ = lax.scan(add_part, jnp.zeros((token_count, D), jnp.float32), (attended_blocks, weight_blocks))
    scaled = mixed_sum * lax.rsqrt(lax.optimization_barrier(jnp.mean(mixed_sum * mixed_sum, axis=1, keepdims=True)) + EPS) * mixer_gain
    return scaled.astype(jnp.bfloat16)

def expert_ref(expert_input, expert_ids, expert_weights, input_gain, w_gate, w_up, w_down, out_gain):
    token_count = expert_input.shape[0]
    inputs_f = expert_input.astype(jnp.float32)
    normed = (inputs_f * lax.rsqrt(lax.optimization_barrier(jnp.mean(inputs_f * inputs_f, axis=1, keepdims=True)) + EPS) * input_gain).astype(jnp.bfloat16)
    padded = jnp.concatenate([normed, jnp.zeros((1, D), jnp.bfloat16)], axis=0)
    flat_ids = expert_ids.reshape(-1)
    pick_count = flat_ids.shape[0]
    top_count = expert_ids.shape[1]
    weight_flat = jnp.concatenate([expert_weights.reshape(-1), jnp.zeros((1,), jnp.float32)])
    slot_total = N_EP * CAP
    block_width = FF // N_TP

    def one_expert(accum, expert_index):
        chosen = flat_ids == expert_index
        position = jnp.cumsum(chosen.astype(jnp.int32)) - 1
        target = jnp.where(chosen, position, slot_total).astype(jnp.int32)
        pick_table = jnp.full((slot_total,), pick_count, jnp.int32).at[target].set(jnp.arange(pick_count, dtype=jnp.int32), mode='drop')
        token_table = (pick_table // top_count).astype(jnp.int32)
        gathered = jnp.take(padded, token_table, axis=0)
        gate_weight = lax.dynamic_index_in_dim(w_gate, expert_index, 0, keepdims=False)
        up_weight = lax.dynamic_index_in_dim(w_up, expert_index, 0, keepdims=False)
        down_weight = lax.dynamic_index_in_dim(w_down, expert_index, 0, keepdims=False)
        gate_pre = jnp.dot(gathered, gate_weight, preferred_element_type=jnp.float32)
        up_pre = jnp.dot(gathered, up_weight, preferred_element_type=jnp.float32)
        hidden = (jax.nn.silu(gate_pre) * up_pre).astype(jnp.bfloat16)
        hidden_blocks = hidden.reshape(slot_total, N_TP, block_width).transpose(1, 0, 2).astype(jnp.float32)
        down_blocks = down_weight.reshape(N_TP, block_width, D).astype(jnp.float32)
        expert_part = jnp.einsum('jsf,jfd->jsd', hidden_blocks, down_blocks).astype(jnp.bfloat16)
        expert_part = lax.optimization_barrier(expert_part)
        expert_rows = lax.optimization_barrier(jnp.sum(expert_part.astype(jnp.float32), axis=0)).astype(jnp.bfloat16)
        weights_now = jnp.take(weight_flat, pick_table)
        accum = accum.at[token_table].add(weights_now[:, None] * expert_rows.astype(jnp.float32), mode='drop')
        return (accum, None)
    combined, _ = lax.scan(one_expert, jnp.zeros((token_count, D), jnp.float32), jnp.arange(EXPERTS, dtype=jnp.int32))
    scaled = combined * lax.rsqrt(lax.optimization_barrier(jnp.mean(combined * combined, axis=1, keepdims=True)) + EPS) * out_gain
    return scaled.astype(jnp.bfloat16)

def reference(query_rows, key_rows, value_rows, query_gain, key_gain, w_out, mixer_gain, expert_input, expert_ids, expert_weights, input_gain, w_gate, w_up, w_down, out_gain):
    mixer_result = mixer_ref(query_rows, key_rows, value_rows, query_gain, key_gain, w_out, mixer_gain)
    moe_result = expert_ref(expert_input, expert_ids, expert_weights, input_gain, w_gate, w_up, w_down, out_gain)
    return (mixer_result, moe_result)
```

```python
import functools
import math

import jax
import jax.numpy as jnp
from jax import lax
from jax.experimental import pallas as pl
from jax.experimental.pallas import tpu as pltpu
from jax.sharding import PartitionSpec as P

D = 2048
GRID = 64
GROUPS = 4
BLOCK_Q = 384
BLOCK_K = 768


EPS = 1e-06
THETA = 10000.0


def turn_half(half_part, position):
    half_width = half_part.shape[-1]
    frequency = THETA ** (-jnp.arange(0, half_width, 2, dtype=jnp.float32) / half_width)
    angles = position[:, None, None] * frequency[None, None, :]
    cosine = jnp.cos(angles)
    sine_part = jnp.sin(angles)
    first_half = half_part[..., : half_width // 2]
    second = half_part[..., half_width // 2 :]
    return jnp.concatenate(
        [first_half * cosine - second * sine_part, second * cosine + first_half * sine_part],
        axis=-1,
    )


def norm_turn(raw_rows, gain_vec, row_offset):
    row_count = raw_rows.shape[0]
    head_dim = gain_vec.shape[0]
    head_count = raw_rows.shape[1] // head_dim
    by_head = raw_rows.astype(jnp.float32).reshape(row_count, head_count, head_dim)
    scaled = (
        by_head * lax.rsqrt(jnp.mean(by_head * by_head, axis=-1, keepdims=True) + EPS) * gain_vec
    )
    position = row_offset + jnp.arange(row_count, dtype=jnp.int32)
    grid_row = (position // GRID).astype(jnp.float32)
    grid_col = (position % GRID).astype(jnp.float32)
    half_dim = head_dim // 2
    turned = jnp.concatenate(
        [turn_half(scaled[..., :half_dim], grid_row), turn_half(scaled[..., half_dim:], grid_col)],
        axis=-1,
    )
    return turned.reshape(row_count, head_count * head_dim).astype(jnp.bfloat16)


def attend_block(scale, block_keys, query, k_ref, k_cols, vt_ref):
    columns, head_dim = query.shape
    steps = k_ref.shape[0] // block_keys

    def step(index, carry):
        top, total, acc = carry
        rows = pl.ds(pl.multiple_of(index * block_keys, block_keys), block_keys)
        scores = (
            lax.dot_general(
                k_ref[rows, k_cols],
                query,
                (((1,), (1,)), ((), ())),
                preferred_element_type=jnp.float32,
            )
            * scale
        )
        new_top = jnp.maximum(top, jnp.max(scores, axis=0, keepdims=True))
        exponent = jnp.exp2(scores - new_top)
        factor = jnp.exp2(top - new_top)
        total = total * factor + jnp.sum(exponent, axis=0, keepdims=True)
        acc = acc * factor + jnp.dot(
            vt_ref[:, rows], exponent.astype(jnp.bfloat16), preferred_element_type=jnp.float32
        )
        return new_top, total, acc

    carry = (
        jnp.full((1, columns), -1e30, jnp.float32),
        jnp.zeros((1, columns), jnp.float32),
        jnp.zeros((head_dim, columns), jnp.float32),
    )
    if steps <= 8:
        for index in range(steps):
            carry = step(index, carry)
    else:
        carry = lax.fori_loop(0, steps, step, carry)
    _, total, acc = carry
    return (acc / total).T.astype(jnp.bfloat16)


def attend_kernel(scale, block_keys, q_ref, k_ref, v_ref, o_ref, vt_ref):
    @pl.when(pl.program_id(1) == 0)
    def _():
        vt_ref[...] = v_ref[...].T

    o_ref[...] = attend_block(scale, block_keys, q_ref[...], k_ref, slice(None), vt_ref)


def attend_send_kernel(
    n_ep, scale, block_keys, packed, out, vt_ref, stage, send_sem, recv_sem, own_sem
):
    me = lax.axis_index("ep")
    row_count = out.shape[0]
    head_dim = vt_ref.shape[0]
    barrier = pltpu.get_barrier_semaphore()
    for offset in range(1, n_ep):
        pl.semaphore_signal(
            barrier,
            inc=1,
            device_id={"ep": lax.rem(me + offset, n_ep)},
            device_id_type=pl.DeviceIdType.MESH,
        )
    pl.semaphore_wait(barrier, n_ep - 1)
    columns = pl.ds(pl.multiple_of(me * head_dim, head_dim), head_dim)

    def send(offset):
        return pltpu.make_async_remote_copy(
            src_ref=stage.at[offset - 1],
            dst_ref=out.at[:, columns],
            send_sem=send_sem.at[offset - 1],
            recv_sem=recv_sem.at[offset - 1],
            device_id={"ep": lax.rem(me + offset, n_ep)},
            device_id_type=pl.DeviceIdType.MESH,
        )

    vt_ref[...] = packed[:, 2 * head_dim : 3 * head_dim].T

    def block(index, carry):
        @pl.when(index > 0)
        def _():
            send(index).start()

        owner = lax.rem(me + index + 1, n_ep)
        rows = pl.ds(pl.multiple_of(owner * row_count, row_count), row_count)
        stage[index] = attend_block(
            scale,
            block_keys,
            packed[rows, 0:head_dim],
            packed,
            slice(head_dim, 2 * head_dim),
            vt_ref,
        )
        return carry

    lax.fori_loop(0, n_ep, block, 0)
    own = pltpu.make_async_copy(stage.at[n_ep - 1], out.at[:, columns], own_sem)
    own.start()
    for offset in range(1, n_ep):
        send(offset).wait()
    own.wait()


def attend_send(packed, n_ep, head_dim):
    tokens = packed.shape[0]
    row_count = tokens // n_ep
    return pl.pallas_call(
        functools.partial(
            attend_send_kernel,
            n_ep,
            head_dim**-0.5 * math.log2(math.e),
            divisor(tokens, BLOCK_K),
        ),
        in_specs=[pl.BlockSpec(memory_space=pltpu.VMEM)],
        out_specs=pl.BlockSpec(memory_space=pltpu.VMEM),
        out_shape=jax.ShapeDtypeStruct((row_count, n_ep * head_dim), jnp.bfloat16),
        scratch_shapes=[
            pltpu.VMEM((head_dim, tokens), jnp.bfloat16),
            pltpu.VMEM((n_ep, row_count, head_dim), jnp.bfloat16),
            pltpu.SemaphoreType.DMA((n_ep - 1,)),
            pltpu.SemaphoreType.DMA((n_ep - 1,)),
            pltpu.SemaphoreType.DMA,
        ],
        compiler_params=pltpu.CompilerParams(collective_id=0, has_side_effects=True),
        cost_estimate=pl.CostEstimate(
            flops=8 * tokens * tokens * head_dim,
            bytes_accessed=8 * tokens * head_dim,
            transcendentals=tokens * tokens,
        ),
        name="attend_send",
    )(packed)


def divisor(size, limit):
    block = limit
    while size % block:
        block -= 128
    return block


def attend(query, key, value, heads, head_dim, group_size, q_col, k_col, v_col):
    tokens = query.shape[0]
    keys = key.shape[0]
    block_q = divisor(tokens, BLOCK_Q)
    block_k = divisor(keys, BLOCK_K)
    flops = 4 * heads * tokens * keys * head_dim
    return pl.pallas_call(
        functools.partial(attend_kernel, head_dim**-0.5 * math.log2(math.e), block_k),
        grid=(heads, tokens // block_q),
        in_specs=[
            pl.BlockSpec((block_q, head_dim), lambda h, i: (i, q_col + h)),
            pl.BlockSpec((keys, head_dim), lambda h, i: (0, k_col + h // group_size)),
            pl.BlockSpec((keys, head_dim), lambda h, i: (0, v_col + h // group_size)),
        ],
        out_specs=pl.BlockSpec((block_q, head_dim), lambda h, i: (i, h)),
        out_shape=jax.ShapeDtypeStruct((tokens, heads * head_dim), jnp.bfloat16),
        scratch_shapes=[pltpu.VMEM((head_dim, keys), jnp.bfloat16)],
        compiler_params=pltpu.CompilerParams(dimension_semantics=("arbitrary", "arbitrary")),
        cost_estimate=pl.CostEstimate(
            flops=2 * flops,
            bytes_accessed=8 * tokens * heads * head_dim,
            transcendentals=heads * tokens * keys,
        ),
        name="attend",
    )(query, key, value)


def mixer_half(query_rows, key_rows, value_rows, query_gain, key_gain, w_out, mixer_gain):
    row_count = query_rows.shape[0]
    head_dim = query_gain.shape[0]
    n_ep = lax.axis_size("ep")
    row_offset = lax.axis_index("ep") * row_count
    query_turned = norm_turn(query_rows, query_gain, row_offset)
    key_turned = norm_turn(key_rows, key_gain, row_offset)
    local_heads = query_rows.shape[1] // head_dim
    group_size = query_rows.shape[1] // key_rows.shape[1]
    if local_heads == n_ep:
        by_head = [
            x.reshape(row_count, -1, head_dim).transpose(1, 0, 2)
            for x in (query_turned, key_turned, value_rows)
        ]
        outgoing = jnp.concatenate(
            [by_head[0]] + [jnp.repeat(x, group_size, axis=0) for x in by_head[1:]], axis=2
        )
        arrived = lax.all_to_all(outgoing, "ep", split_axis=0, concat_axis=0, tiled=True)
        packed = arrived.reshape(n_ep * row_count, 3 * head_dim)
        attended = attend_send(packed, n_ep, head_dim)
    else:
        key_all = lax.all_gather(key_turned, "ep", axis=0, tiled=True)
        value_all = lax.all_gather(value_rows, "ep", axis=0, tiled=True)
        attended = attend(
            query_turned, key_all, value_all, local_heads, head_dim, group_size, 0, 0, 0
        )
    mixed_sum = lax.psum_scatter(
        jnp.dot(attended, w_out, preferred_element_type=jnp.float32).astype(jnp.bfloat16),
        "tp",
        scatter_dimension=0,
        tiled=True,
    ).astype(jnp.float32)
    scaled = (
        mixed_sum
        * lax.rsqrt(jnp.mean(mixed_sum * mixed_sum, axis=1, keepdims=True) + EPS)
        * mixer_gain
    )
    return scaled.astype(jnp.bfloat16)


def expert_half(
    expert_input, expert_ids, expert_weights, input_gain, w_gate, w_up, w_down, out_gain
):
    row_count, width = expert_input.shape
    top_count = expert_ids.shape[1]
    n_tp = lax.axis_size("tp")
    expert_total = w_gate.shape[0] * lax.axis_size("ep")
    inner_count = expert_total // GROUPS
    capacity = 3 * row_count // (4 * inner_count)
    slots = expert_total * capacity
    inputs_f = expert_input.astype(jnp.float32)
    normed = (
        inputs_f
        * lax.rsqrt(jnp.mean(inputs_f * inputs_f, axis=1, keepdims=True) + EPS)
        * input_gain
    ).astype(jnp.bfloat16)
    row_index = jnp.arange(row_count, dtype=jnp.int32)
    before = row_index[None, :] < row_index[:, None]
    slot_index = jnp.arange(slots, dtype=jnp.int32)
    slot_of = []
    for k in range(top_count):
        same = jnp.zeros((row_count, row_count), bool)
        for other in range(top_count):
            same = same | (expert_ids[:, k][:, None] == expert_ids[:, other][None, :])
        rank = jnp.sum((same & before).astype(jnp.int32), axis=1)
        slot_of.append(expert_ids[:, k] * capacity + rank)
    chosen = [slot_index[:, None] == slot[None, :] for slot in slot_of]
    picker = functools.reduce(jnp.logical_or, chosen).astype(jnp.bfloat16)
    share = width // n_tp
    own = lax.dynamic_slice_in_dim(normed, lax.axis_index("tp") * share, share, axis=1)
    outgoing = jnp.dot(picker, own, preferred_element_type=jnp.float32).astype(jnp.bfloat16)
    arrived = lax.all_to_all(
        outgoing.reshape(expert_total, capacity, share),
        "ep",
        split_axis=0,
        concat_axis=0,
        tiled=True,
    ).reshape(slots, share)
    shares = lax.all_gather(arrived, "tp", axis=0, tiled=False)
    arrived = jnp.concatenate([shares[j] for j in range(n_tp)], axis=1)
    gate_pre = jnp.dot(arrived, w_gate[0], preferred_element_type=jnp.float32)
    up_pre = jnp.dot(arrived, w_up[0], preferred_element_type=jnp.float32)
    hidden = (jax.nn.silu(gate_pre) * up_pre).astype(jnp.bfloat16)
    partial_term = jnp.dot(hidden, w_down[0], preferred_element_type=jnp.float32)
    summed = lax.psum_scatter(
        partial_term.astype(jnp.bfloat16), "tp", scatter_dimension=1, tiled=True
    )
    returned = lax.all_to_all(summed, "ep", split_axis=0, concat_axis=0, tiled=True)
    combined = jnp.zeros((row_count, returned.shape[1]), jnp.float32)
    for k in range(top_count):
        select = (slot_of[k][:, None] == slot_index[None, :]).astype(jnp.bfloat16)
        picked = jnp.dot(select, returned, preferred_element_type=jnp.float32)
        combined = combined + picked * expert_weights[:, k][:, None]
    squares = lax.psum(jnp.sum(combined * combined, axis=1), "tp")
    scaled = combined * lax.rsqrt(squares / D + EPS)[:, None] * out_gain
    return scaled.astype(jnp.bfloat16)


MESH_ID = pl.DeviceIdType.MESH
KEY_STEP = 768
FF_STEP = 256


def remote(src, dst, send_sem, recv_sem, ep, tp):
    return pltpu.make_async_remote_copy(
        src_ref=src,
        dst_ref=dst,
        send_sem=send_sem,
        recv_sem=recv_sem,
        device_id={"ep": ep, "tp": tp},
        device_id_type=MESH_ID,
    )


def aligned(index, size):
    return pl.ds(pl.multiple_of(index * size, size), size)


def turn_rows(raw, gain, cosine, sine, low_lane):
    rows = raw.astype(jnp.float32)
    mean = jnp.mean(rows * rows, axis=1, keepdims=True)
    rows = rows * lax.rsqrt(mean + EPS) * gain
    head_dim = rows.shape[1]
    quarter = head_dim // 4
    swapped = jnp.where(
        low_lane, pltpu.roll(rows, head_dim - quarter, 1), pltpu.roll(rows, quarter, 1)
    )
    return (rows * cosine + swapped * sine).astype(jnp.bfloat16)


def attend_heads(query, k_ref, vt_ref, first_done):
    columns, head_dim = query.shape
    steps = k_ref.shape[0] // KEY_STEP
    top = jnp.full((1, columns), -1e30, jnp.float32)
    total = jnp.zeros((1, columns), jnp.float32)
    acc = jnp.zeros((head_dim, columns), jnp.float32)
    for index in range(steps):
        rows = slice(index * KEY_STEP, (index + 1) * KEY_STEP)
        scores = lax.dot_general(
            k_ref[rows, :], query, (((1,), (1,)), ((), ())), preferred_element_type=jnp.float32
        )
        new_top = jnp.maximum(top, jnp.max(scores, axis=0, keepdims=True))
        exponent = jnp.exp2(scores - new_top)
        factor = jnp.exp2(top - new_top)
        total = total * factor + jnp.sum(exponent, axis=0, keepdims=True)
        acc = acc * factor + jnp.dot(
            vt_ref[:, rows], exponent.astype(jnp.bfloat16), preferred_element_type=jnp.float32
        )
        top = new_top
    return (acc / total).T.astype(jnp.bfloat16)


def layer_kernel(
    n_z,
    n_x,
    n_tp,
    cap,
    q_ref,
    k_ref,
    v_ref,
    cos_ref,
    sin_ref,
    q_gain,
    k_gain,
    mixer_gain,
    x_ref,
    ids_ref,
    weight_ref,
    in_gain,
    out_gain,
    w_gate,
    w_up,
    w_down,
    w_out,
    mixer_out,
    moe_out,
    wg,
    wu,
    wd,
    wo,
    q_stage,
    k_stage,
    v_stage,
    k_all,
    vt_all,
    q_all,
    o_stage,
    o_all,
    picker,
    x_stage,
    x_all,
    hidden,
    part_send,
    part_keep,
    part_recv,
    pair_send,
    pair_recv,
    rows_out,
    returned,
    squares_send,
    squares_recv,
    head_send,
    head_keep,
    head_recv,
    head_pair,
    head_last,
    w_sem,
    own_sem,
    mz_s,
    mz_r,
    mx_s,
    mx_r,
    my_s,
    my_r,
    mc_s,
    mc_r,
    k_s,
    k_r,
    vz_s,
    vz_r,
    kx_s,
    kx_r,
    vx_s,
    vx_r,
    q_s,
    q_r,
    o_s,
    o_r,
    pc_s,
    pc_r,
    py_s,
    py_r,
    ret_s,
    ret_r,
    sq_s,
    sq_r,
    hc_s,
    hc_r,
    hy_s,
    hy_r,
):
    me = lax.axis_index("ep")
    t = lax.axis_index("tp")
    z = me // n_x
    x = lax.rem(me, n_x)
    other_x = 1 - x
    core = t + 1 - 2 * lax.rem(t, 2)
    across = lax.rem(t + 2, n_tp)
    diagonal = lax.rem(core + 2, n_tp)
    x_peer = z * n_x + other_x

    def plane(offset):
        return lax.rem(z + offset, n_z)

    def source(offset):
        return lax.rem(z + n_z - offset, n_z)

    weights = [
        pltpu.make_async_copy(w_gate.at[0], wg, w_sem.at[0]),
        pltpu.make_async_copy(w_up.at[0], wu, w_sem.at[1]),
        pltpu.make_async_copy(w_down.at[0], wd, w_sem.at[2]),
        pltpu.make_async_copy(w_out, wo, w_sem.at[3]),
    ]
    for copy in weights:
        copy.start()

    barrier = pltpu.get_barrier_semaphore()
    greeted = [(plane(o) * n_x + x, t) for o in range(1, n_z)]
    greeted += [(plane(o) * n_x + other_x, t) for o in range(n_z)]
    greeted += [(me, core), (me, across), (me, diagonal)]
    for ep, tp in greeted:
        pl.semaphore_signal(barrier, inc=1, device_id={"ep": ep, "tp": tp}, device_id_type=MESH_ID)

    rows, width = x_ref.shape
    share = width // n_tp
    own_cols = aligned(t, share)
    group_rows = n_z * cap
    x_full = x_ref[...].astype(jnp.float32)
    scale = lax.rsqrt(jnp.mean(x_full * x_full, axis=1, keepdims=True) + EPS)
    normed = (x_ref[:, own_cols].astype(jnp.float32) * scale * in_gain[:, own_cols]).astype(
        jnp.bfloat16
    )
    first_id = ids_ref[:, 0:1]
    lane = lax.broadcasted_iota(jnp.int32, (rows, 128), 1)
    in_group = (first_id >= lane * n_x) & (first_id < lane * n_x + n_x)
    row_at = lax.broadcasted_iota(jnp.int32, (rows, rows), 0)
    col_at = lax.broadcasted_iota(jnp.int32, (rows, rows), 1)
    earlier = jnp.where(col_at < row_at, 1.0, 0.0).astype(jnp.bfloat16)
    counts = jnp.dot(
        earlier,
        jnp.where(in_group, 1.0, 0.0).astype(jnp.bfloat16),
        preferred_element_type=jnp.float32,
    )
    slot = jnp.sum(
        jnp.where(in_group, counts + (lane * cap).astype(jnp.float32), 0.0), axis=1, keepdims=True
    )
    slot_at = lax.broadcasted_iota(jnp.int32, (rows, group_rows), 1).astype(jnp.float32)
    picker[...] = jnp.where(slot_at == slot, 1.0, 0.0).astype(jnp.bfloat16)
    x_stage[...] = lax.dot_general(
        picker[...], normed, (((0,), (0,)), ((), ())), preferred_element_type=jnp.float32
    ).astype(jnp.bfloat16)
    pl.semaphore_wait(barrier, len(greeted))

    def chunk_at(region, index):
        return x_all.at[region, aligned(index, cap), own_cols]

    sent = []

    def go(copy):
        copy.start()
        sent.append(copy)
        return copy

    own_rows = x_stage.at[aligned(z, cap), :]
    moe_z = []
    for o in (2, 1, 3):
        moe_z.append(
            go(
                remote(
                    x_stage.at[aligned(plane(o), cap), :],
                    chunk_at(0, z),
                    mz_s.at[o - 1],
                    mz_r.at[o - 1],
                    plane(o) * n_x + x,
                    t,
                )
            )
        )
    own_x = pltpu.make_async_copy(own_rows, chunk_at(0, z), own_sem.at[0])
    own_x.start()
    moe_x = [go(remote(own_rows, chunk_at(1, z), mx_s.at[0], mx_r.at[0], x_peer, t))]
    moe_y = [[go(remote(own_rows, chunk_at(0, z), my_s.at[0, 0], my_r.at[0, 0], me, across))], []]

    tokens, kv_width = k_ref.shape
    head_dim = q_gain.shape[1]
    q_width = q_ref.shape[1] // n_z
    lanes = lax.broadcasted_iota(jnp.int32, (tokens, head_dim), 1)
    low_lane = lax.rem(lanes, head_dim // 2) < head_dim // 4
    cosine, sine = cos_ref[...], sin_ref[...]
    for g in range(n_z):
        cols = slice(g * head_dim, (g + 1) * head_dim)
        k_stage[g] = turn_rows(k_ref[:, cols], k_gain[...], cosine, sine, low_lane)
        v_stage[g] = v_ref[:, cols].T

    def k_at(region, index):
        return k_all.at[aligned(region * n_z + index, tokens), :]

    def v_at(region, index):
        return vt_all.at[:, aligned(region * n_z + index, tokens)]

    kv_z = []
    for o in (2, 1, 3):
        to = plane(o)
        kv_z.append(
            (
                go(remote(k_stage.at[to], k_at(0, z), k_s.at[o - 1], k_r.at[o - 1], to * n_x + x, t)),
                go(
                    remote(
                        v_stage.at[to], v_at(0, z), vz_s.at[o - 1], vz_r.at[o - 1], to * n_x + x, t
                    )
                ),
            )
        )
    own_k = pltpu.make_async_copy(k_stage.at[z], k_at(0, z), own_sem.at[1])
    own_v = pltpu.make_async_copy(v_stage.at[z], v_at(0, z), own_sem.at[2])
    own_k.start()
    own_v.start()
    kv_x = [
        go(remote(k_stage.at[z], k_at(1, z), kx_s.at[0], kx_r.at[0], x_peer, t)),
        go(remote(v_stage.at[z], v_at(1, z), vx_s.at[0], vx_r.at[0], x_peer, t)),
    ]

    heads = q_width // head_dim
    to_exponent = head_dim**-0.5 * math.log2(math.e)
    for g in range(n_z):
        for h in range(heads):
            cols = slice((g * heads + h) * head_dim, (g * heads + h + 1) * head_dim)
            q_stage[g, :, h * head_dim : (h + 1) * head_dim] = turn_rows(
                q_ref[:, cols], q_gain[...] * to_exponent, cosine, sine, low_lane
            )
    for o in (1, 2, 3):
        to = plane(o)
        go(remote(q_stage.at[to], q_all.at[z], q_s.at[o - 1], q_r.at[o - 1], to * n_x + x, t))
    own_q = pltpu.make_async_copy(q_stage.at[z], q_all.at[z], own_sem.at[3])
    own_q.start()

    for copy, o in zip(moe_z, (2, 1, 3)):
        copy.wait_recv()
        here = chunk_at(0, source(o))
        moe_y[0].append(go(remote(here, here, my_s.at[0, o], my_r.at[0, o], me, across)))
        moe_x.append(
            go(remote(here, chunk_at(1, source(o)), mx_s.at[o], mx_r.at[o], x_peer, t))
        )
    own_x.wait()

    def cols_at(region, tp):
        return x_all.at[region, :, aligned(tp, share)]

    moe_c = [[], []]
    moe_c[0].append(
        go(remote(cols_at(0, t), cols_at(0, t), mc_s.at[0, 0], mc_r.at[0, 0], me, core))
    )
    for copy, o in zip(moe_x, (0, 2, 1, 3)):
        copy.wait_recv()
        here = chunk_at(1, source(o))
        moe_y[1].append(go(remote(here, here, my_s.at[1, o], my_r.at[1, o], me, across)))
    moe_c[1].append(
        go(remote(cols_at(1, t), cols_at(1, t), mc_s.at[1, 0], mc_r.at[1, 0], me, core))
    )
    for copy in moe_y[0]:
        copy.wait_recv()
    moe_c[0].append(
        go(remote(cols_at(0, across), cols_at(0, across), mc_s.at[0, 1], mc_r.at[0, 1], me, core))
    )

    def forward_keys(index, o):
        key_copy, value_copy = kv_z[index]
        key_copy.wait_recv()
        kv_x.append(
            go(
                remote(
                    k_at(0, source(o)), k_at(1, source(o)), kx_s.at[o], kx_r.at[o], x_peer, t
                )
            )
        )
        value_copy.wait_recv()
        kv_x.append(
            go(
                remote(
                    v_at(0, source(o)), v_at(1, source(o)), vx_s.at[o], vx_r.at[o], x_peer, t
                )
            )
        )

    blocks = (core, diagonal, t, across)
    inner_width = wg.shape[1]

    def experts(region):
        for copy in moe_c[region]:
            copy.wait_recv()
        if region == 0:
            weights[0].wait()
            weights[1].wait()

        def pre(index, carry):
            cols = aligned(index, FF_STEP)
            rows_in = x_all[region]
            gate = jnp.dot(rows_in, wg[:, cols], preferred_element_type=jnp.float32)
            up = jnp.dot(rows_in, wu[:, cols], preferred_element_type=jnp.float32)
            hidden[:, cols] = (gate / (1.0 + jnp.exp(-gate)) * up).astype(jnp.bfloat16)
            return carry

        lax.fori_loop(0, inner_width // FF_STEP, pre, 0)
        if region == 0:
            weights[2].wait()
        for index, block in enumerate(blocks):
            part = jnp.dot(
                hidden[...], wd[:, aligned(block, share)], preferred_element_type=jnp.float32
            ).astype(jnp.bfloat16)
            if index < 2:
                part_send[region, index] = part
                go(
                    remote(
                        part_send.at[region, index],
                        part_recv.at[region, index],
                        pc_s.at[region, index],
                        pc_r.at[region, index],
                        me,
                        core,
                    )
                )
            else:
                part_keep[region, index - 2] = part

    def part_copy(region, index):
        return remote(
            part_send.at[region, index],
            part_recv.at[region, index],
            pc_s.at[region, index],
            pc_r.at[region, index],
            me,
            core,
        )

    def pair_copy(region):
        return remote(
            pair_send.at[region], pair_recv.at[region], py_s.at[region], py_r.at[region], me, across
        )

    def pair(region):
        part_copy(region, 1).wait_recv()
        pair_send[region] = (
            part_keep[region, 1].astype(jnp.float32) + part_recv[region, 1].astype(jnp.float32)
        ).astype(jnp.bfloat16)
        sent.append(pair_copy(region))
        sent[-1].start()

    experts(0)
    pair(0)
    forward_keys(0, 2)
    forward_keys(1, 1)
    for copy in moe_y[1]:
        copy.wait_recv()
    moe_c[1].append(
        go(remote(cols_at(1, across), cols_at(1, across), mc_s.at[1, 1], mc_r.at[1, 1], me, core))
    )
    forward_keys(2, 3)
    experts(1)
    pair(1)

    def return_copy(region, o):
        to = plane(o)
        return remote(
            rows_out.at[region, aligned(to, cap), :],
            returned.at[aligned(x * n_z + z, cap), :],
            ret_s.at[region, o],
            ret_r.at[region, o],
            to * n_x + (x if region == 0 else other_x),
            t,
        )

    own_return = pltpu.make_async_copy(
        rows_out.at[0, aligned(z, cap), :],
        returned.at[aligned(x * n_z + z, cap), :],
        own_sem.at[4],
    )
    returns = [(0, o) for o in range(1, n_z)] + [(1, o) for o in range(n_z)]

    def send_back():
        for region in range(n_x):
            part_copy(region, 0).wait_recv()
            pair_copy(region).wait_recv()
            rows_out[region] = (
                part_keep[region, 0].astype(jnp.float32)
                + part_recv[region, 0].astype(jnp.float32)
                + pair_recv[region].astype(jnp.float32)
            ).astype(jnp.bfloat16)
        for region, o in returns:
            return_copy(region, o).start()
        own_return.start()

    for copy in kv_x:
        copy.wait_recv()
    own_k.wait()
    own_v.wait()
    own_q.wait()

    def output_copy(o):
        to = plane(o)
        return remote(
            o_stage.at[to],
            o_all.at[:, aligned(z, q_width)],
            o_s.at[o - 1],
            o_r.at[o - 1],
            to * n_x + x,
            t,
        )

    def block(index, carry):
        o = index + 1
        to = plane(o)

        @pl.when(o < n_z)
        def _():
            back = n_z - o
            remote(
                q_stage.at[to], q_all.at[to], q_s.at[back - 1], q_r.at[back - 1], me, core
            ).wait_recv()

        for h in range(heads):
            cols = slice(h * head_dim, (h + 1) * head_dim)
            o_stage[to, :, cols] = attend_heads(q_all[to, :, cols], k_all, vt_all, None)

        @pl.when(o < n_z)
        def _():
            output_copy(o).start()

        @pl.when(o == n_z // 2)
        def _():
            send_back()

        return carry

    lax.fori_loop(0, n_z, block, 0)
    own_o = pltpu.make_async_copy(
        o_stage.at[z], o_all.at[:, aligned(z, q_width)], own_sem.at[5]
    )
    own_o.start()
    weights[3].wait()
    for o in range(1, n_z):
        output_copy(o).wait_recv()
    own_o.wait()

    own_tokens = tokens // n_tp
    out_width = wo.shape[1]

    def project(first, second, into):
        taken = jnp.concatenate(
            [o_all[aligned(first, own_tokens), :], o_all[aligned(second, own_tokens), :]], axis=0
        )

        def columns(index, carry):
            cols = aligned(index, 512)
            part = jnp.dot(taken, wo[:, cols], preferred_element_type=jnp.float32).astype(
                jnp.bfloat16
            )
            into[0, :, cols] = part[:own_tokens]
            into[1, :, cols] = part[own_tokens:]
            return carry

        lax.fori_loop(0, out_width // 512, columns, 0)

    project(core, diagonal, head_send)
    head_c = [
        go(remote(head_send.at[i], head_recv.at[i], hc_s.at[i], hc_r.at[i], me, core))
        for i in (1, 0)
    ]
    project(t, across, head_keep)
    head_c[0].wait_recv()
    head_pair[...] = (
        head_keep[1].astype(jnp.float32) + head_recv[1].astype(jnp.float32)
    ).astype(jnp.bfloat16)
    head_y = go(remote(head_pair, head_last, hy_s.at[0], hy_r.at[0], me, across))

    for region, o in returns:
        return_copy(region, o).wait_recv()
    own_return.wait()
    picks = picker[...]
    ids = ids_ref[...]
    mix = weight_ref[...]
    combined = jnp.zeros((rows, share), jnp.float32)
    for parity in range(n_x):
        gathered = jnp.dot(
            picks,
            returned[parity * group_rows : (parity + 1) * group_rows, :],
            preferred_element_type=jnp.float32,
        )
        factor = jnp.sum(
            jnp.where(lax.rem(ids, n_x) == parity, mix, 0.0), axis=1, keepdims=True
        )
        combined = combined + gathered * factor
    squares = jnp.sum(combined * combined, axis=1, keepdims=True)
    squares_send[...] = jnp.broadcast_to(squares, (rows, 128)).T[0:8, :]
    square_copies = [
        go(remote(squares_send, squares_recv.at[i], sq_s.at[i], sq_r.at[i], me, tp))
        for i, tp in enumerate((core, across, diagonal))
    ]
    for copy in square_copies:
        copy.wait_recv()
    all_squares = squares_send[...] + squares_recv[0] + squares_recv[1] + squares_recv[2]
    spread = jnp.broadcast_to(all_squares[0:1, :], (128, rows)).T[:, 0:1]
    moe_out[...] = (combined * lax.rsqrt(spread / width + EPS) * out_gain[...]).astype(
        jnp.bfloat16
    )

    head_c[1].wait_recv()
    head_y.wait_recv()
    mixed = (
        head_keep[0].astype(jnp.float32)
        + head_recv[0].astype(jnp.float32)
        + head_last[...].astype(jnp.float32)
    )
    mean = jnp.mean(mixed * mixed, axis=1, keepdims=True)
    mixer_out[...] = (mixed * lax.rsqrt(mean + EPS) * mixer_gain[...]).astype(jnp.bfloat16)

    for copy in sent:
        copy.wait_send()
    for o in range(1, n_z):
        output_copy(o).wait_send()
    for region, o in returns:
        return_copy(region, o).wait_send()


def turn_tables(row_count, row_offset, head_dim):
    position = row_offset + jnp.arange(row_count, dtype=jnp.int32)
    half_width = head_dim // 2
    frequency = THETA ** (-jnp.arange(0, half_width, 2, dtype=jnp.float32) / half_width)
    row_angle = (position // GRID).astype(jnp.float32)[:, None] * frequency[None, :]
    col_angle = (position % GRID).astype(jnp.float32)[:, None] * frequency[None, :]
    angles = jnp.concatenate([row_angle, row_angle, col_angle, col_angle], axis=1)
    lane = jnp.arange(head_dim, dtype=jnp.int32)[None, :]
    sign = jnp.where(lane % half_width < half_width // 2, -1.0, 1.0)
    return jnp.cos(angles), jnp.sin(angles) * sign


def layer(
    n_z,
    n_x,
    query_rows,
    key_rows,
    value_rows,
    query_gain,
    key_gain,
    w_out,
    mixer_gain,
    expert_input,
    expert_ids,
    expert_weights,
    input_gain,
    w_gate,
    w_up,
    w_down,
    out_gain,
):
    n_tp = lax.axis_size("tp")
    tokens = query_rows.shape[0]
    head_dim = query_gain.shape[0]
    rows, width = expert_input.shape
    share = width // n_tp
    inner = w_gate.shape[2]
    q_width = query_rows.shape[1] // n_z
    cap = -(-(3 * rows // (4 * n_x)) // 16) * 16
    cosine, sine = turn_tables(tokens, lax.axis_index("ep") * tokens, head_dim)
    bf16, f32 = jnp.bfloat16, jnp.float32
    vmem = pl.BlockSpec(memory_space=pltpu.VMEM)
    hbm = pl.BlockSpec(memory_space=pl.ANY)
    dma = pltpu.SemaphoreType.DMA
    group_rows = n_z * cap
    own_tokens = tokens // n_tp
    far = n_z - 1
    scratch = [
        pltpu.VMEM(w_gate.shape[1:], bf16),
        pltpu.VMEM(w_up.shape[1:], bf16),
        pltpu.VMEM(w_down.shape[1:], bf16),
        pltpu.VMEM(w_out.shape, bf16),
        pltpu.VMEM((n_z, tokens, q_width), bf16),
        pltpu.VMEM((n_z, tokens, head_dim), bf16),
        pltpu.VMEM((n_z, head_dim, tokens), bf16),
        pltpu.VMEM((n_x * n_z * tokens, head_dim), bf16),
        pltpu.VMEM((head_dim, n_x * n_z * tokens), bf16),
        pltpu.VMEM((n_z, tokens, q_width), bf16),
        pltpu.VMEM((n_z, tokens, q_width), bf16),
        pltpu.VMEM((tokens, n_z * q_width), bf16),
        pltpu.VMEM((rows, group_rows), bf16),
        pltpu.VMEM((group_rows, share), bf16),
        pltpu.VMEM((n_x, group_rows, width), bf16),
        pltpu.VMEM((group_rows, inner), bf16),
        pltpu.VMEM((n_x, 2, group_rows, share), bf16),
        pltpu.VMEM((n_x, 2, group_rows, share), bf16),
        pltpu.VMEM((n_x, 2, group_rows, share), bf16),
        pltpu.VMEM((n_x, group_rows, share), bf16),
        pltpu.VMEM((n_x, group_rows, share), bf16),
        pltpu.VMEM((n_x, group_rows, share), bf16),
        pltpu.VMEM((n_x * group_rows, share), bf16),
        pltpu.VMEM((8, rows), f32),
        pltpu.VMEM((3, 8, rows), f32),
        pltpu.VMEM((2, own_tokens, width), bf16),
        pltpu.VMEM((2, own_tokens, width), bf16),
        pltpu.VMEM((2, own_tokens, width), bf16),
        pltpu.VMEM((own_tokens, width), bf16),
        pltpu.VMEM((own_tokens, width), bf16),
        dma((4,)),
        dma((6,)),
    ]
    for shape in (
        (far,),
        (n_z,),
        (n_x, n_z),
        (n_x, 2),
        (far,),
        (far,),
        (n_z,),
        (n_z,),
        (far,),
        (far,),
        (n_x, 2),
        (n_x,),
        (n_x, n_z),
        (3,),
        (2,),
        (1,),
    ):
        scratch += [dma(shape), dma(shape)]
    return pl.pallas_call(
        functools.partial(layer_kernel, n_z, n_x, n_tp, cap),
        in_specs=[vmem] * 13 + [hbm] * 4,
        out_specs=(vmem, vmem),
        out_shape=(
            jax.ShapeDtypeStruct((own_tokens, width), bf16),
            jax.ShapeDtypeStruct((rows, share), bf16),
        ),
        scratch_shapes=scratch,
        compiler_params=pltpu.CompilerParams(
            collective_id=0, has_side_effects=True, vmem_limit_bytes=60 * 1024 * 1024
        ),
        name="layer",
    )(
        query_rows,
        key_rows,
        value_rows,
        cosine,
        sine,
        query_gain[None, :],
        key_gain[None, :],
        mixer_gain[None, :],
        expert_input,
        expert_ids,
        expert_weights,
        input_gain[None, :],
        out_gain[None, :],
        w_gate,
        w_up,
        w_down,
        w_out,
    )


def per_device(
    query_rows,
    key_rows,
    value_rows,
    query_gain,
    key_gain,
    w_out,
    mixer_gain,
    expert_input,
    expert_ids,
    expert_weights,
    input_gain,
    w_gate,
    w_up,
    w_down,
    out_gain,
):
    n_ep = lax.axis_size("ep")
    n_z = key_rows.shape[1] // query_gain.shape[0]
    n_x = w_gate.shape[0] * n_ep // GROUPS
    if (
        n_z == GROUPS
        and n_z * n_x == n_ep
        and n_x == 2
        and expert_ids.shape[1] == n_x
        and w_gate.shape[0] == 1
        and lax.axis_size("tp") == 4
    ):
        return layer(
            n_z,
            n_x,
            query_rows,
            key_rows,
            value_rows,
            query_gain,
            key_gain,
            w_out,
            mixer_gain,
            expert_input,
            expert_ids,
            expert_weights,
            input_gain,
            w_gate,
            w_up,
            w_down,
            out_gain,
        )
    mixer_result = mixer_half(
        query_rows, key_rows, value_rows, query_gain, key_gain, w_out, mixer_gain
    )
    moe_result = expert_half(
        expert_input, expert_ids, expert_weights, input_gain, w_gate, w_up, w_down, out_gain
    )
    return (mixer_result, moe_result)


def solution(mesh):
    return jax.shard_map(
        per_device,
        mesh=mesh,
        in_specs=(
            P("ep", "tp"),
            P("ep", "tp"),
            P("ep", "tp"),
            P(),
            P(),
            P("tp", None),
            P(),
            P("ep", None),
            P("ep", None),
            P("ep", None),
            P(),
            P("ep", None, "tp"),
            P("ep", None, "tp"),
            P("ep", "tp", None),
            P("tp"),
        ),
        out_specs=(P(("ep", "tp"), None), P("ep", "tp")),
        check_vma=False,
    )
```

```python
import functools
import math

import jax
import jax.numpy as jnp
import numpy as np
from jax import lax
from jax.experimental import pallas as pl
from jax.experimental.pallas import tpu as pltpu
from jax.sharding import PartitionSpec as P

D = 2048
GRID = 64
GROUPS = 4
BLOCK_Q = 384
BLOCK_K = 768


EPS = 1e-06
THETA = 10000.0


def turn_half(half_part, position):
    half_width = half_part.shape[-1]
    frequency = THETA ** (-jnp.arange(0, half_width, 2, dtype=jnp.float32) / half_width)
    angles = position[:, None, None] * frequency[None, None, :]
    cosine = jnp.cos(angles)
    sine_part = jnp.sin(angles)
    first_half = half_part[..., : half_width // 2]
    second = half_part[..., half_width // 2 :]
    return jnp.concatenate(
        [first_half * cosine - second * sine_part, second * cosine + first_half * sine_part],
        axis=-1,
    )


def norm_turn(raw_rows, gain_vec, row_offset):
    row_count = raw_rows.shape[0]
    head_dim = gain_vec.shape[0]
    head_count = raw_rows.shape[1] // head_dim
    by_head = raw_rows.astype(jnp.float32).reshape(row_count, head_count, head_dim)
    scaled = (
        by_head * lax.rsqrt(jnp.mean(by_head * by_head, axis=-1, keepdims=True) + EPS) * gain_vec
    )
    position = row_offset + jnp.arange(row_count, dtype=jnp.int32)
    grid_row = (position // GRID).astype(jnp.float32)
    grid_col = (position % GRID).astype(jnp.float32)
    half_dim = head_dim // 2
    turned = jnp.concatenate(
        [turn_half(scaled[..., :half_dim], grid_row), turn_half(scaled[..., half_dim:], grid_col)],
        axis=-1,
    )
    return turned.reshape(row_count, head_count * head_dim).astype(jnp.bfloat16)


def attend_block(scale, block_keys, query, k_ref, k_cols, vt_ref):
    columns, head_dim = query.shape
    steps = k_ref.shape[0] // block_keys

    def step(index, carry):
        top, total, acc = carry
        rows = pl.ds(pl.multiple_of(index * block_keys, block_keys), block_keys)
        scores = (
            lax.dot_general(
                k_ref[rows, k_cols],
                query,
                (((1,), (1,)), ((), ())),
                preferred_element_type=jnp.float32,
            )
            * scale
        )
        new_top = jnp.maximum(top, jnp.max(scores, axis=0, keepdims=True))
        exponent = jnp.exp2(scores - new_top)
        factor = jnp.exp2(top - new_top)
        total = total * factor + jnp.sum(exponent, axis=0, keepdims=True)
        acc = acc * factor + jnp.dot(
            vt_ref[:, rows], exponent.astype(jnp.bfloat16), preferred_element_type=jnp.float32
        )
        return new_top, total, acc

    carry = (
        jnp.full((1, columns), -1e30, jnp.float32),
        jnp.zeros((1, columns), jnp.float32),
        jnp.zeros((head_dim, columns), jnp.float32),
    )
    if steps <= 8:
        for index in range(steps):
            carry = step(index, carry)
    else:
        carry = lax.fori_loop(0, steps, step, carry)
    _, total, acc = carry
    return (acc / total).T.astype(jnp.bfloat16)


def attend_kernel(scale, block_keys, q_ref, k_ref, v_ref, o_ref, vt_ref):
    @pl.when(pl.program_id(1) == 0)
    def _():
        vt_ref[...] = v_ref[...].T

    o_ref[...] = attend_block(scale, block_keys, q_ref[...], k_ref, slice(None), vt_ref)


def attend_send_kernel(
    n_ep, scale, block_keys, packed, out, vt_ref, stage, send_sem, recv_sem, own_sem
):
    me = lax.axis_index("ep")
    row_count = out.shape[0]
    head_dim = vt_ref.shape[0]
    barrier = pltpu.get_barrier_semaphore()
    for offset in range(1, n_ep):
        pl.semaphore_signal(
            barrier,
            inc=1,
            device_id={"ep": lax.rem(me + offset, n_ep)},
            device_id_type=pl.DeviceIdType.MESH,
        )
    pl.semaphore_wait(barrier, n_ep - 1)
    columns = pl.ds(pl.multiple_of(me * head_dim, head_dim), head_dim)

    def send(offset):
        return pltpu.make_async_remote_copy(
            src_ref=stage.at[offset - 1],
            dst_ref=out.at[:, columns],
            send_sem=send_sem.at[offset - 1],
            recv_sem=recv_sem.at[offset - 1],
            device_id={"ep": lax.rem(me + offset, n_ep)},
            device_id_type=pl.DeviceIdType.MESH,
        )

    vt_ref[...] = packed[:, 2 * head_dim : 3 * head_dim].T

    def block(index, carry):
        @pl.when(index > 0)
        def _():
            send(index).start()

        owner = lax.rem(me + index + 1, n_ep)
        rows = pl.ds(pl.multiple_of(owner * row_count, row_count), row_count)
        stage[index] = attend_block(
            scale,
            block_keys,
            packed[rows, 0:head_dim],
            packed,
            slice(head_dim, 2 * head_dim),
            vt_ref,
        )
        return carry

    lax.fori_loop(0, n_ep, block, 0)
    own = pltpu.make_async_copy(stage.at[n_ep - 1], out.at[:, columns], own_sem)
    own.start()
    for offset in range(1, n_ep):
        send(offset).wait()
    own.wait()


def attend_send(packed, n_ep, head_dim):
    tokens = packed.shape[0]
    row_count = tokens // n_ep
    return pl.pallas_call(
        functools.partial(
            attend_send_kernel,
            n_ep,
            head_dim**-0.5 * math.log2(math.e),
            divisor(tokens, BLOCK_K),
        ),
        in_specs=[pl.BlockSpec(memory_space=pltpu.VMEM)],
        out_specs=pl.BlockSpec(memory_space=pltpu.VMEM),
        out_shape=jax.ShapeDtypeStruct((row_count, n_ep * head_dim), jnp.bfloat16),
        scratch_shapes=[
            pltpu.VMEM((head_dim, tokens), jnp.bfloat16),
            pltpu.VMEM((n_ep, row_count, head_dim), jnp.bfloat16),
            pltpu.SemaphoreType.DMA((n_ep - 1,)),
            pltpu.SemaphoreType.DMA((n_ep - 1,)),
            pltpu.SemaphoreType.DMA,
        ],
        compiler_params=pltpu.CompilerParams(collective_id=0, has_side_effects=True),
        cost_estimate=pl.CostEstimate(
            flops=8 * tokens * tokens * head_dim,
            bytes_accessed=8 * tokens * head_dim,
            transcendentals=tokens * tokens,
        ),
        name="attend_send",
    )(packed)


def divisor(size, limit):
    block = limit
    while size % block:
        block -= 128
    return block


def attend(query, key, value, heads, head_dim, group_size, q_col, k_col, v_col):
    tokens = query.shape[0]
    keys = key.shape[0]
    block_q = divisor(tokens, BLOCK_Q)
    block_k = divisor(keys, BLOCK_K)
    flops = 4 * heads * tokens * keys * head_dim
    return pl.pallas_call(
        functools.partial(attend_kernel, head_dim**-0.5 * math.log2(math.e), block_k),
        grid=(heads, tokens // block_q),
        in_specs=[
            pl.BlockSpec((block_q, head_dim), lambda h, i: (i, q_col + h)),
            pl.BlockSpec((keys, head_dim), lambda h, i: (0, k_col + h // group_size)),
            pl.BlockSpec((keys, head_dim), lambda h, i: (0, v_col + h // group_size)),
        ],
        out_specs=pl.BlockSpec((block_q, head_dim), lambda h, i: (i, h)),
        out_shape=jax.ShapeDtypeStruct((tokens, heads * head_dim), jnp.bfloat16),
        scratch_shapes=[pltpu.VMEM((head_dim, keys), jnp.bfloat16)],
        compiler_params=pltpu.CompilerParams(dimension_semantics=("arbitrary", "arbitrary")),
        cost_estimate=pl.CostEstimate(
            flops=2 * flops,
            bytes_accessed=8 * tokens * heads * head_dim,
            transcendentals=heads * tokens * keys,
        ),
        name="attend",
    )(query, key, value)


def mixer_half(query_rows, key_rows, value_rows, query_gain, key_gain, w_out, mixer_gain):
    row_count = query_rows.shape[0]
    head_dim = query_gain.shape[0]
    n_ep = lax.axis_size("ep")
    row_offset = lax.axis_index("ep") * row_count
    query_turned = norm_turn(query_rows, query_gain, row_offset)
    key_turned = norm_turn(key_rows, key_gain, row_offset)
    local_heads = query_rows.shape[1] // head_dim
    group_size = query_rows.shape[1] // key_rows.shape[1]
    if local_heads == n_ep:
        by_head = [
            x.reshape(row_count, -1, head_dim).transpose(1, 0, 2)
            for x in (query_turned, key_turned, value_rows)
        ]
        outgoing = jnp.concatenate(
            [by_head[0]] + [jnp.repeat(x, group_size, axis=0) for x in by_head[1:]], axis=2
        )
        arrived = lax.all_to_all(outgoing, "ep", split_axis=0, concat_axis=0, tiled=True)
        packed = arrived.reshape(n_ep * row_count, 3 * head_dim)
        attended = attend_send(packed, n_ep, head_dim)
    else:
        key_all = lax.all_gather(key_turned, "ep", axis=0, tiled=True)
        value_all = lax.all_gather(value_rows, "ep", axis=0, tiled=True)
        attended = attend(
            query_turned, key_all, value_all, local_heads, head_dim, group_size, 0, 0, 0
        )
    mixed_sum = lax.psum_scatter(
        jnp.dot(attended, w_out, preferred_element_type=jnp.float32).astype(jnp.bfloat16),
        "tp",
        scatter_dimension=0,
        tiled=True,
    ).astype(jnp.float32)
    scaled = (
        mixed_sum
        * lax.rsqrt(jnp.mean(mixed_sum * mixed_sum, axis=1, keepdims=True) + EPS)
        * mixer_gain
    )
    return scaled.astype(jnp.bfloat16)


def expert_half(
    expert_input, expert_ids, expert_weights, input_gain, w_gate, w_up, w_down, out_gain
):
    row_count, width = expert_input.shape
    top_count = expert_ids.shape[1]
    n_tp = lax.axis_size("tp")
    expert_total = w_gate.shape[0] * lax.axis_size("ep")
    inner_count = expert_total // GROUPS
    capacity = 3 * row_count // (4 * inner_count)
    slots = expert_total * capacity
    inputs_f = expert_input.astype(jnp.float32)
    normed = (
        inputs_f
        * lax.rsqrt(jnp.mean(inputs_f * inputs_f, axis=1, keepdims=True) + EPS)
        * input_gain
    ).astype(jnp.bfloat16)
    row_index = jnp.arange(row_count, dtype=jnp.int32)
    before = row_index[None, :] < row_index[:, None]
    slot_index = jnp.arange(slots, dtype=jnp.int32)
    slot_of = []
    for k in range(top_count):
        same = jnp.zeros((row_count, row_count), bool)
        for other in range(top_count):
            same = same | (expert_ids[:, k][:, None] == expert_ids[:, other][None, :])
        rank = jnp.sum((same & before).astype(jnp.int32), axis=1)
        slot_of.append(expert_ids[:, k] * capacity + rank)
    chosen = [slot_index[:, None] == slot[None, :] for slot in slot_of]
    picker = functools.reduce(jnp.logical_or, chosen).astype(jnp.bfloat16)
    share = width // n_tp
    own = lax.dynamic_slice_in_dim(normed, lax.axis_index("tp") * share, share, axis=1)
    outgoing = jnp.dot(picker, own, preferred_element_type=jnp.float32).astype(jnp.bfloat16)
    arrived = lax.all_to_all(
        outgoing.reshape(expert_total, capacity, share),
        "ep",
        split_axis=0,
        concat_axis=0,
        tiled=True,
    ).reshape(slots, share)
    shares = lax.all_gather(arrived, "tp", axis=0, tiled=False)
    arrived = jnp.concatenate([shares[j] for j in range(n_tp)], axis=1)
    gate_pre = jnp.dot(arrived, w_gate[0], preferred_element_type=jnp.float32)
    up_pre = jnp.dot(arrived, w_up[0], preferred_element_type=jnp.float32)
    hidden = (jax.nn.silu(gate_pre) * up_pre).astype(jnp.bfloat16)
    partial_term = jnp.dot(hidden, w_down[0], preferred_element_type=jnp.float32)
    summed = lax.psum_scatter(
        partial_term.astype(jnp.bfloat16), "tp", scatter_dimension=1, tiled=True
    )
    returned = lax.all_to_all(summed, "ep", split_axis=0, concat_axis=0, tiled=True)
    combined = jnp.zeros((row_count, returned.shape[1]), jnp.float32)
    for k in range(top_count):
        select = (slot_of[k][:, None] == slot_index[None, :]).astype(jnp.bfloat16)
        picked = jnp.dot(select, returned, preferred_element_type=jnp.float32)
        combined = combined + picked * expert_weights[:, k][:, None]
    squares = lax.psum(jnp.sum(combined * combined, axis=1), "tp")
    scaled = combined * lax.rsqrt(squares / D + EPS)[:, None] * out_gain
    return scaled.astype(jnp.bfloat16)


MESH_ID = pl.DeviceIdType.MESH
FF_STEP = 256


def remote(src, dst, send_sem, recv_sem, ep, tp):
    return pltpu.make_async_remote_copy(
        src_ref=src,
        dst_ref=dst,
        send_sem=send_sem,
        recv_sem=recv_sem,
        device_id={"ep": ep, "tp": tp},
        device_id_type=MESH_ID,
    )


def aligned(index, size):
    return pl.ds(pl.multiple_of(index * size, size), size)


def turn_rows(raw, gain, cosine, sine, low_lane):
    rows = raw.astype(jnp.float32)
    mean = jnp.mean(rows * rows, axis=1, keepdims=True)
    rows = rows * lax.rsqrt(mean + EPS) * gain
    head_dim = rows.shape[1]
    quarter = head_dim // 4
    swapped = jnp.where(
        low_lane, pltpu.roll(rows, head_dim - quarter, 1), pltpu.roll(rows, quarter, 1)
    )
    return (rows * cosine + swapped * sine).astype(jnp.bfloat16)


def attend_keys(query, keys, values_t, state):
    top, total, acc = state
    scores = lax.dot_general(
        keys, query, (((1,), (1,)), ((), ())), preferred_element_type=jnp.float32
    )
    new_top = jnp.maximum(top, jnp.max(scores, axis=0, keepdims=True))
    exponent = jnp.exp2(scores - new_top)
    factor = jnp.exp2(top - new_top)
    total = total * factor + jnp.sum(exponent, axis=0, keepdims=True)
    acc = acc * factor + jnp.dot(
        values_t, exponent.astype(jnp.bfloat16), preferred_element_type=jnp.float32
    )
    return new_top, total, acc


def layer_kernel(
    n_ep,
    n_x,
    n_tp,
    cap,
    q_ref,
    k_ref,
    v_ref,
    row_table,
    col_table,
    q_gain,
    k_gain,
    mixer_gain,
    x_ref,
    ids_ref,
    weight_ref,
    in_gain,
    out_gain,
    w_gate,
    w_up,
    w_down,
    w_out,
    mixer_out,
    moe_out,
    wg,
    wu,
    wd,
    wo,
    q_stage,
    k_stage,
    v_stage,
    k_all,
    vt_all,
    q_all,
    tops,
    totals,
    accs,
    o_stage,
    o_all,
    picker,
    x_stage,
    x_all,
    mix_stage,
    mix_all,
    hidden,
    part_send,
    part_keep,
    part_recv,
    pair_send,
    pair_recv,
    rows_out,
    rows_in,
    joined,
    returned,
    squares_send,
    squares_recv,
    head_part,
    head_recv,
    head_pair,
    head_last,
    w_sem,
    own_sem,
    mz_s,
    mz_r,
    mw_s,
    mw_r,
    mx_s,
    mx_r,
    my_s,
    my_r,
    mc_s,
    mc_r,
    k_s,
    k_r,
    v_s,
    v_r,
    kf_s,
    kf_r,
    vf_s,
    vf_r,
    q_s,
    q_r,
    o_s,
    o_r,
    pc_s,
    pc_r,
    py_s,
    py_r,
    jx_s,
    jx_r,
    ret_s,
    ret_r,
    sq_s,
    sq_r,
    hc_s,
    hc_r,
    hy_s,
    hy_r,
):
    me = lax.axis_index("ep")
    t = lax.axis_index("tp")
    n_z = n_ep // n_x
    slots = n_z
    planes = slots // n_x
    z = me // n_x
    x = lax.rem(me, n_x)
    other_x = 1 - x
    core = t + 1 - 2 * lax.rem(t, 2)
    across = lax.rem(t + 2, n_tp)
    diagonal = lax.rem(core + 2, n_tp)
    x_peer = z * n_x + other_x
    block = me // slots
    slot = lax.rem(me, slots)
    level = slot // n_x
    far = level + (1 - block) - 2 * level * (1 - block)

    def plane(offset):
        return lax.rem(z + offset, n_z)

    def source(offset):
        return lax.rem(z + n_z - offset, n_z)

    def peer(index):
        flip_level = 1 - index // 2
        flip_x = lax.rem((index + 1) // 2, 2)
        to_level = level + flip_level - 2 * level * flip_level
        to_x = x + flip_x - 2 * x * flip_x
        return to_level * n_x + to_x

    sent = []

    def go(copy):
        copy.start()
        sent.append(copy)
        return copy

    weights = [
        pltpu.make_async_copy(w_gate.at[0], wg, w_sem.at[0]),
        pltpu.make_async_copy(w_up.at[0], wu, w_sem.at[1]),
        pltpu.make_async_copy(w_down.at[0], wd, w_sem.at[2]),
        pltpu.make_async_copy(w_out, wo, w_sem.at[3]),
    ]
    for copy in weights:
        copy.start()

    barrier = pltpu.get_barrier_semaphore()
    greeted = [(plane(o) * n_x + x, t) for o in range(1, n_z)]
    greeted += [(block * slots + peer(i), t) for i in (1, 2)]
    greeted += [((1 - block) * slots + peer(i), t) for i in (1, 2)]
    greeted += [(me, core), (me, across), (me, diagonal)]
    for ep, tp in greeted:
        pl.semaphore_signal(barrier, inc=1, device_id={"ep": ep, "tp": tp}, device_id_type=MESH_ID)

    rows, width = x_ref.shape
    share = width // n_tp
    own_cols = aligned(t, share)
    group_rows = n_z * cap
    x_full = x_ref[...].astype(jnp.float32)
    scale = lax.rsqrt(jnp.mean(x_full * x_full, axis=1, keepdims=True) + EPS)
    normed = (x_ref[:, own_cols].astype(jnp.float32) * scale * in_gain[:, own_cols]).astype(
        jnp.bfloat16
    )
    id_rows = ids_ref[...]
    first_id = jnp.broadcast_to(id_rows[0:1, :].astype(jnp.float32), (128, rows)).T
    lane = lax.broadcasted_iota(jnp.int32, (rows, 128), 1).astype(jnp.float32)
    in_group = (first_id >= lane * n_x) & (first_id < lane * n_x + n_x)
    row_at = lax.broadcasted_iota(jnp.int32, (rows, rows), 0)
    col_at = lax.broadcasted_iota(jnp.int32, (rows, rows), 1)
    earlier = jnp.where(col_at < row_at, 1.0, 0.0).astype(jnp.bfloat16)
    counts = jnp.dot(
        earlier,
        jnp.where(in_group, 1.0, 0.0).astype(jnp.bfloat16),
        preferred_element_type=jnp.float32,
    )
    place = jnp.sum(jnp.where(in_group, counts + lane * cap, 0.0), axis=1, keepdims=True)
    place_at = lax.broadcasted_iota(jnp.int32, (rows, group_rows), 1).astype(jnp.float32)
    picks = jnp.where(place_at == place, 1.0, 0.0)
    picker[...] = picks.astype(jnp.bfloat16)
    x_stage[...] = lax.dot_general(
        picker[...], normed, (((0,), (0,)), ((), ())), preferred_element_type=jnp.float32
    ).astype(jnp.bfloat16)
    odd = lax.rem(id_rows, n_x) == 1
    mix = weight_ref[...]
    second = jnp.sum(jnp.where(odd, mix, 0.0), axis=0, keepdims=True)
    first = jnp.sum(jnp.where(odd, 0.0, mix), axis=0, keepdims=True)
    at_row = lax.broadcasted_iota(jnp.int32, (8, rows), 0)
    both = jnp.where(at_row == 0, first, jnp.where(at_row == 1, second, 0.0))
    placed = jnp.dot(
        both, picks, preferred_element_type=jnp.float32, precision=lax.Precision.HIGHEST
    )
    for g in range(n_z):
        mix_stage[g, :, 0:cap] = placed[:, g * cap : (g + 1) * cap]

    tokens = k_ref.shape[0]
    head_dim = q_gain.shape[1]
    heads = q_ref.shape[1] // (slots * head_dim)
    own_tokens = tokens // n_tp
    half_own = own_tokens // 2
    half_tokens = tokens // 2
    lanes = lax.broadcasted_iota(jnp.int32, (tokens, head_dim), 1)
    low_lane = lax.rem(lanes, head_dim // 2) < head_dim // 4
    grid_rows = tokens // GRID
    by_row = lax.broadcasted_iota(jnp.int32, (GRID, head_dim), 1) < head_dim // 2

    def table(which):
        return jnp.concatenate(
            [
                jnp.where(
                    by_row, row_table[which, pl.ds(me * grid_rows + r, 1), :], col_table[which]
                )
                for r in range(grid_rows)
            ],
            axis=0,
        )

    cosine, sine = table(0), table(1)
    for g in range(slots):
        cols = slice(g * head_dim, (g + 1) * head_dim)
        k_stage[g] = turn_rows(k_ref[:, cols], k_gain[...], cosine, sine, low_lane)
        v_stage[g] = v_ref[:, cols].T
    pl.semaphore_wait(barrier, len(greeted))

    def chunk_at(region, index):
        return x_all.at[region, aligned(index, cap), own_cols]

    own_rows = x_stage.at[aligned(z, cap), :]
    moe_z = []
    for o in (2, 1, 3):
        to = plane(o)
        moe_z.append(
            go(
                remote(
                    x_stage.at[aligned(to, cap), :],
                    chunk_at(0, z),
                    mz_s.at[o - 1],
                    mz_r.at[o - 1],
                    to * n_x + x,
                    t,
                )
            )
        )
    moe_w = []
    for o in (2, 1, 3):
        to = plane(o)
        moe_w.append(
            go(
                remote(
                    mix_stage.at[to], mix_all.at[z], mw_s.at[o - 1], mw_r.at[o - 1], to * n_x + x, t
                )
            )
        )
    own_x = pltpu.make_async_copy(own_rows, chunk_at(0, z), own_sem.at[0])
    own_x.start()
    own_mix = pltpu.make_async_copy(mix_stage.at[z], mix_all.at[z], own_sem.at[1])
    own_mix.start()
    moe_y = [[go(remote(own_rows, chunk_at(0, z), my_s.at[0, 0], my_r.at[0, 0], me, across))], []]
    moe_x = [go(remote(own_rows, chunk_at(1, z), mx_s.at[0], mx_r.at[0], x_peer, t))]

    def k_at(index):
        return k_all.at[aligned(index, tokens), :]

    def v_at(index):
        return vt_all.at[:, aligned(index, tokens)]

    def near_keys(i, index):
        to = peer(i)
        ep = block * slots + to
        return (
            go(remote(k_stage.at[to], k_at(index), k_s.at[i], k_r.at[i], ep, t)),
            go(remote(v_stage.at[to], v_at(index), v_s.at[i], v_r.at[i], ep, t)),
        )

    def near_queries(i):
        to = peer(i)
        ep = block * slots + to
        go(remote(q_stage.at[to], q_all.at[slot], q_s.at[i], q_r.at[i], ep, t))

    to_exponent = head_dim**-0.5 * math.log2(math.e)
    for g in range(slots):
        for h in range(heads):
            cols = slice((g * heads + h) * head_dim, (g * heads + h + 1) * head_dim)
            turned = turn_rows(q_ref[:, cols], q_gain[...] * to_exponent, cosine, sine, low_lane)
            for part in range(2):
                for owner in range(n_tp):
                    first_row = h * tokens + part * half_tokens + owner * half_own
                    from_row = owner * own_tokens + part * half_own
                    q_stage[g, first_row : first_row + half_own, :] = turned[
                        from_row : from_row + half_own
                    ]
    own_copies = [
        pltpu.make_async_copy(k_stage.at[slot], k_at(0), own_sem.at[2]),
        pltpu.make_async_copy(v_stage.at[slot], v_at(0), own_sem.at[3]),
        pltpu.make_async_copy(q_stage.at[slot], q_all.at[slot], own_sem.at[4]),
    ]
    for copy in own_copies:
        copy.start()

    for copy, o in zip(moe_z, (2, 1, 3)):
        copy.wait_recv()
        here = chunk_at(0, source(o))
        moe_y[0].append(go(remote(here, here, my_s.at[0, o], my_r.at[0, o], me, across)))
        moe_x.append(go(remote(here, chunk_at(1, source(o)), mx_s.at[o], mx_r.at[o], x_peer, t)))
    own_x.wait()

    straight_keys = near_keys(0, 1)
    near_queries(0)

    def far_copies(order, cross):
        flip = 1 - order - far + 2 * order * far
        to_level = level + flip - 2 * level * flip
        to = to_level * n_x + (other_x if cross else x)
        ep = (1 - block) * slots + to
        at = planes * (1 + 2 * cross) + far
        send, arrive = planes * cross + order, planes * cross + far
        return (
            remote(k_stage.at[to], k_at(at), kf_s.at[send], kf_r.at[arrive], ep, t),
            remote(v_stage.at[to], v_at(at), vf_s.at[send], vf_r.at[arrive], ep, t),
        )

    def send_far(cross):
        for order in range(planes):
            for copy in far_copies(order, cross):
                copy.start()

    def wait_far(cross):
        for order in range(planes):
            at, arrive = planes * (1 + 2 * cross) + order, planes * cross + order
            remote(
                k_stage.at[slot], k_at(at), kf_s.at[0], kf_r.at[arrive], me, core
            ).wait_recv()
            remote(
                v_stage.at[slot], v_at(at), vf_s.at[0], vf_r.at[arrive], me, core
            ).wait_recv()

    send_far(0)

    def cols_at(region, tp):
        return x_all.at[region, :, aligned(tp, share)]

    def to_core(region, index, tp):
        return go(
            remote(
                cols_at(region, tp),
                cols_at(region, tp),
                mc_s.at[region, index],
                mc_r.at[region, index],
                me,
                core,
            )
        )

    moe_c = [[to_core(0, 0, t)], []]
    for copy, o in zip(moe_x, (0, 2, 1, 3)):
        copy.wait_recv()
        here = chunk_at(1, source(o))
        moe_y[1].append(go(remote(here, here, my_s.at[1, o], my_r.at[1, o], me, across)))
    moe_c[1].append(to_core(1, 0, t))
    near_queries(2)
    near_queries(1)
    crossed_keys = near_keys(2, slots) + near_keys(1, slots + 1)
    send_far(1)
    for copy in moe_y[0]:
        copy.wait_recv()
    moe_c[0].append(to_core(0, 1, across))

    blocks = (core, diagonal, t, across)
    inner_width = wg.shape[1]

    def part_copy(region, index):
        return remote(
            part_send.at[region, index],
            part_recv.at[region, index],
            pc_s.at[region, index],
            pc_r.at[region, index],
            me,
            core,
        )

    def experts(region):
        for copy in moe_c[region]:
            copy.wait_recv()
        if region == 0:
            weights[0].wait()
            weights[1].wait()

        def pre(index, carry):
            cols = aligned(index, FF_STEP)
            rows_now = x_all[region]
            gate = jnp.dot(rows_now, wg[:, cols], preferred_element_type=jnp.float32)
            up = jnp.dot(rows_now, wu[:, cols], preferred_element_type=jnp.float32)
            hidden[:, cols] = (gate / (1.0 + jnp.exp(-gate)) * up).astype(jnp.bfloat16)
            return carry

        lax.fori_loop(0, inner_width // FF_STEP, pre, 0)
        if region == 0:
            weights[2].wait()
        for index in (1, 0, 3, 2):
            part = jnp.dot(
                hidden[...],
                wd[:, aligned(blocks[index], share)],
                preferred_element_type=jnp.float32,
            ).astype(jnp.bfloat16)
            if index < 2:
                part_send[region, index] = part
                go(part_copy(region, index))
            else:
                part_keep[region, index - 2] = part

    def pair_copy(region):
        return remote(
            pair_send.at[region], pair_recv.at[region], py_s.at[region], py_r.at[region], me, across
        )

    def pair(region):
        part_copy(region, 1).wait_recv()
        pair_send[region] = (
            part_keep[region, 1].astype(jnp.float32) + part_recv[region, 1].astype(jnp.float32)
        ).astype(jnp.bfloat16)
        pair_copy(region).start()

    experts(0)
    step = 2 * tokens
    queries = heads * tokens

    def key_step(index):
        return slice(index * step, (index + 1) * step)

    def load_state(to):
        return tops[to, 0:1, :], totals[to, 0:1, :], accs[to]

    def save_state(to, state):
        tops[to, 0:1, :], totals[to, 0:1, :], accs[to] = state

    def own_block(turn, carry):
        index = lax.rem(turn + slots - 1, slots)
        to = peer(index)

        @pl.when(index < slots - 1)
        def _():
            remote(
                q_stage.at[to], q_all.at[to], q_s.at[index], q_r.at[index], me, core
            ).wait_recv()

        state = (
            jnp.full((1, queries), -1e30, jnp.float32),
            jnp.zeros((1, queries), jnp.float32),
            jnp.zeros((head_dim, queries), jnp.float32),
        )
        for s in range(slots // 2):
            state = attend_keys(q_all[to], k_all[key_step(s), :], vt_all[:, key_step(s)], state)
        save_state(to, state)

        @pl.when(turn == 0)
        def _():
            pair(1)

        return carry

    for copy in moe_y[1]:
        copy.wait_recv()
    moe_c[1].append(to_core(1, 1, across))
    pair(0)
    experts(1)
    for copy in own_copies:
        copy.wait()
    for copy in straight_keys:
        copy.wait_recv()
    wait_far(0)
    lax.fori_loop(0, slots, own_block, 0)

    join = remote(rows_out.at[1], rows_in, jx_s.at[0], jx_r.at[0], x_peer, t)
    sent.append(join)

    def expert_rows():
        for region in (1, 0):
            part_copy(region, 0).wait_recv()
            pair_copy(region).wait_recv()
            rows_out[region] = (
                part_keep[region, 0].astype(jnp.float32)
                + part_recv[region, 0].astype(jnp.float32)
                + pair_recv[region].astype(jnp.float32)
            ).astype(jnp.bfloat16)
            if region == 1:
                join.start()

    for copy in crossed_keys:
        copy.wait_recv()

    def near_block(index, carry):
        to = peer(index)
        s = slots // 2
        save_state(
            to,
            attend_keys(q_all[to], k_all[key_step(s), :], vt_all[:, key_step(s)], load_state(to)),
        )
        @pl.when(index == 1)
        def _():
            expert_rows()

        return carry

    lax.fori_loop(0, slots, near_block, 0)

    def output_copy(index, part):
        to = peer(index)
        at = slice(part * half_tokens, (part + 1) * half_tokens)
        return remote(
            o_stage.at[to, :, at, :],
            o_all.at[pl.ds(slot * heads, heads), at, :],
            o_s.at[part, index],
            o_r.at[part, index],
            block * slots + to,
            t,
        )

    def last_block(index, carry):
        to = peer(index)
        s = slots // 2 + 1
        _, total, acc = attend_keys(
            q_all[to], k_all[key_step(s), :], vt_all[:, key_step(s)], load_state(to)
        )
        out = (acc / total).T.astype(jnp.bfloat16)
        for h in range(heads):
            o_stage[to, h] = out[h * tokens : (h + 1) * tokens]

        @pl.when(index == 0)
        def _():
            output_copy(0, 0).start()

        @pl.when(index == 1)
        def _():
            output_copy(1, 0).start()
            output_copy(0, 1).start()
            output_copy(1, 1).start()

        @pl.when(index == 2)
        def _():
            output_copy(2, 0).start()
            output_copy(2, 1).start()

        return carry

    wait_far(1)
    lax.fori_loop(0, slots, last_block, 0)
    own_o = pltpu.make_async_copy(
        o_stage.at[slot], o_all.at[pl.ds(slot * heads, heads)], own_sem.at[6]
    )
    own_o.start()

    weights[3].wait()
    own_o.wait()

    out_width = wo.shape[1]
    all_heads = slots * heads

    pieces = 2
    piece_width = out_width // pieces

    def project(part):
        at = slice(part * half_tokens, (part + 1) * half_tokens)
        taken = jnp.concatenate([o_all[h, at, :] for h in range(all_heads)], axis=1)
        copies = []
        for piece in range(pieces):

            def columns(index, carry):
                cols = aligned(index, 512)
                out = jnp.dot(taken, wo[:, cols], preferred_element_type=jnp.float32).astype(
                    jnp.bfloat16
                )
                for owner in range(n_tp):
                    head_part[part, owner, :, cols] = out[owner * half_own : (owner + 1) * half_own]
                return carry

            lax.fori_loop(
                piece * piece_width // 512, (piece + 1) * piece_width // 512, columns, 0
            )
            cols = slice(piece * piece_width, (piece + 1) * piece_width)
            copies.append(
                [
                    go(
                        remote(
                            head_part.at[part, to, :, cols],
                            head_recv.at[part, i, :, cols],
                            hc_s.at[part, piece, i],
                            hc_r.at[part, piece, i],
                            me,
                            core,
                        )
                    )
                    for i, to in ((1, diagonal), (0, core))
                ]
            )
        return copies

    def to_across(part, copies):
        sums = []
        for piece in range(pieces):
            cols = slice(piece * piece_width, (piece + 1) * piece_width)
            copies[piece][0].wait_recv()
            head_pair[part, :, cols] = (
                head_part[part, across, :, cols].astype(jnp.float32)
                + head_recv[part, 1, :, cols].astype(jnp.float32)
            ).astype(jnp.bfloat16)
            sums.append(
                go(
                    remote(
                        head_pair.at[part, :, cols],
                        head_last.at[part, :, cols],
                        hy_s.at[part, piece],
                        hy_r.at[part, piece],
                        me,
                        across,
                    )
                )
            )
        return sums

    for i in (0, 1, 2):
        output_copy(i, 0).wait_recv()
    first_half = project(0)
    first_y = to_across(0, first_half)
    for copy in moe_w:
        copy.wait_recv()
    own_mix.wait()
    join.wait_recv()
    mine_first = x == 0
    for g in range(n_z):
        mix_cols = mix_all[g].T
        here = slice(g * cap, (g + 1) * cap)
        mine = rows_out[0, here, :].astype(jnp.float32)
        theirs = rows_in[here, :].astype(jnp.float32)
        first_w, second_w = mix_cols[0:cap, 0:1], mix_cols[0:cap, 1:2]
        joined[here, :] = (
            mine * jnp.where(mine_first, first_w, second_w)
            + theirs * jnp.where(mine_first, second_w, first_w)
        ).astype(jnp.bfloat16)

    def back_at():
        return returned.at[aligned(z, cap), :]

    own_return = pltpu.make_async_copy(joined.at[aligned(z, cap), :], back_at(), own_sem.at[5])
    own_return.start()
    returns = []
    for o in (2, 1, 3):
        to = plane(o)
        returns.append(
            go(
                remote(
                    joined.at[aligned(to, cap), :],
                    back_at(),
                    ret_s.at[o - 1],
                    ret_r.at[o - 1],
                    to * n_x + x,
                    t,
                )
            )
        )
    for i in (0, 1, 2):
        output_copy(i, 1).wait_recv()
    second_half = project(1)
    second_y = to_across(1, second_half)
    for copy in returns:
        copy.wait_recv()
    own_return.wait()
    combined = jnp.dot(picker[...], returned[...], preferred_element_type=jnp.float32)
    squares = jnp.sum(combined * combined, axis=1, keepdims=True)
    squares_send[...] = jnp.broadcast_to(squares, (rows, 128)).T[0:8, :]
    square_copies = [
        go(remote(squares_send, squares_recv.at[i], sq_s.at[i], sq_r.at[i], me, tp))
        for i, tp in enumerate((core, across, diagonal))
    ]

    for copy in square_copies:
        copy.wait_recv()
    all_squares = squares_send[...] + squares_recv[0] + squares_recv[1] + squares_recv[2]
    spread = jnp.broadcast_to(all_squares[0:1, :], (128, rows)).T[:, 0:1]
    moe_out[...] = (combined * lax.rsqrt(spread / width + EPS) * out_gain[...]).astype(
        jnp.bfloat16
    )

    for part, copies, last in ((0, first_half, first_y), (1, second_half, second_y)):
        for piece in range(pieces):
            copies[piece][1].wait_recv()
            last[piece].wait_recv()
        mixed = (
            head_part[part, t].astype(jnp.float32)
            + head_recv[part, 0].astype(jnp.float32)
            + head_last[part].astype(jnp.float32)
        )
        mean = jnp.mean(mixed * mixed, axis=1, keepdims=True)
        mixer_out[part * half_own : (part + 1) * half_own, :] = (
            mixed * lax.rsqrt(mean + EPS) * mixer_gain[...]
        ).astype(jnp.bfloat16)

    for copy in sent:
        copy.wait_send()
    for region in range(n_x):
        pair_copy(region).wait_send()
    for cross in range(n_x):
        for order in range(planes):
            for copy in far_copies(order, cross):
                copy.wait_send()
    for i in (0, 1, 2):
        for part in range(2):
            output_copy(i, part).wait_send()


def turn_tables(row_count, head_dim):
    half_width = head_dim // 2
    steps = np.arange(0, half_width, 2, dtype=np.float32) / np.float32(half_width)
    frequency = np.float32(THETA) ** -steps
    sign = np.where(np.arange(half_width) < half_width // 2, -1.0, 1.0)
    tables = []
    for count in (row_count, GRID):
        angles = np.arange(count, dtype=np.float32)[:, None] * frequency[None, :]
        angles = np.tile(angles, (1, 2)).astype(np.float64)
        both = np.stack([np.cos(angles), np.sin(angles) * sign])
        tables.append(np.tile(both, (1, 1, 2)).astype(np.float32))
    return tables


def layer(
    n_x,
    query_rows,
    key_rows,
    value_rows,
    query_gain,
    key_gain,
    w_out,
    mixer_gain,
    expert_input,
    expert_ids,
    expert_weights,
    input_gain,
    w_gate,
    w_up,
    w_down,
    out_gain,
):
    n_ep = lax.axis_size("ep")
    n_tp = lax.axis_size("tp")
    n_z = n_ep // n_x
    slots = n_z
    tokens = query_rows.shape[0]
    head_dim = query_gain.shape[0]
    heads = query_rows.shape[1] // (slots * head_dim)
    rows, width = expert_input.shape
    share = width // n_tp
    inner = w_gate.shape[2]
    cap = -(-(3 * rows // (4 * n_x)) // 16) * 16
    row_table, col_table = turn_tables(n_ep * tokens // GRID, head_dim)
    bf16, f32 = jnp.bfloat16, jnp.float32
    vmem = pl.BlockSpec(memory_space=pltpu.VMEM)
    hbm = pl.BlockSpec(memory_space=pl.ANY)
    dma = pltpu.SemaphoreType.DMA
    group_rows = n_z * cap
    own_tokens = tokens // n_tp
    half_own = own_tokens // 2
    queries = heads * tokens
    keys = n_ep * tokens
    scratch = [
        pltpu.VMEM(w_gate.shape[1:], bf16),
        pltpu.VMEM(w_up.shape[1:], bf16),
        pltpu.VMEM(w_down.shape[1:], bf16),
        pltpu.VMEM(w_out.shape, bf16),
        pltpu.VMEM((slots, queries, head_dim), bf16),
        pltpu.VMEM((slots, tokens, head_dim), bf16),
        pltpu.VMEM((slots, head_dim, tokens), bf16),
        pltpu.VMEM((keys, head_dim), bf16),
        pltpu.VMEM((head_dim, keys), bf16),
        pltpu.VMEM((slots, queries, head_dim), bf16),
        pltpu.VMEM((slots, 8, queries), f32),
        pltpu.VMEM((slots, 8, queries), f32),
        pltpu.VMEM((slots, head_dim, queries), f32),
        pltpu.VMEM((slots, heads, tokens, head_dim), bf16),
        pltpu.VMEM((slots * heads, tokens, head_dim), bf16),
        pltpu.VMEM((rows, group_rows), bf16),
        pltpu.VMEM((group_rows, share), bf16),
        pltpu.VMEM((n_x, group_rows, width), bf16),
        pltpu.VMEM((n_z, 8, 128), f32),
        pltpu.VMEM((n_z, 8, 128), f32),
        pltpu.VMEM((group_rows, inner), bf16),
        pltpu.VMEM((n_x, 2, group_rows, share), bf16),
        pltpu.VMEM((n_x, 2, group_rows, share), bf16),
        pltpu.VMEM((n_x, 2, group_rows, share), bf16),
        pltpu.VMEM((n_x, group_rows, share), bf16),
        pltpu.VMEM((n_x, group_rows, share), bf16),
        pltpu.VMEM((n_x, group_rows, share), bf16),
        pltpu.VMEM((group_rows, share), bf16),
        pltpu.VMEM((group_rows, share), bf16),
        pltpu.VMEM((group_rows, share), bf16),
        pltpu.VMEM((8, rows), f32),
        pltpu.VMEM((3, 8, rows), f32),
        pltpu.VMEM((2, n_tp, half_own, width), bf16),
        pltpu.VMEM((2, 2, half_own, width), bf16),
        pltpu.VMEM((2, half_own, width), bf16),
        pltpu.VMEM((2, half_own, width), bf16),
        dma((4,)),
        dma((7,)),
    ]
    for shape in (
        (n_z - 1,),
        (n_z - 1,),
        (n_z,),
        (n_x, n_z),
        (n_x, 2),
        (slots - 1,),
        (slots - 1,),
        (slots,),
        (slots,),
        (slots - 1,),
        (2, slots - 1),
        (n_x, 2),
        (n_x,),
        (1,),
        (n_z - 1,),
        (3,),
        (2, 2, 2),
        (2, 2),
    ):
        scratch += [dma(shape), dma(shape)]
    return pl.pallas_call(
        functools.partial(layer_kernel, n_ep, n_x, n_tp, cap),
        in_specs=[vmem] * 13 + [hbm] * 4,
        out_specs=(vmem, vmem),
        out_shape=(
            jax.ShapeDtypeStruct((own_tokens, width), bf16),
            jax.ShapeDtypeStruct((rows, share), bf16),
        ),
        scratch_shapes=scratch,
        compiler_params=pltpu.CompilerParams(
            collective_id=0, has_side_effects=True, vmem_limit_bytes=60 * 1024 * 1024
        ),
        name="layer",
    )(
        query_rows,
        key_rows,
        value_rows,
        jnp.asarray(row_table),
        jnp.asarray(col_table),
        query_gain[None, :],
        key_gain[None, :],
        mixer_gain[None, :],
        expert_input,
        expert_ids.T,
        expert_weights.T,
        input_gain[None, :],
        out_gain[None, :],
        w_gate,
        w_up,
        w_down,
        w_out,
    )


def per_device(
    query_rows,
    key_rows,
    value_rows,
    query_gain,
    key_gain,
    w_out,
    mixer_gain,
    expert_input,
    expert_ids,
    expert_weights,
    input_gain,
    w_gate,
    w_up,
    w_down,
    out_gain,
):
    n_ep = lax.axis_size("ep")
    n_x = w_gate.shape[0] * n_ep // GROUPS
    kv_heads = key_rows.shape[1] // query_gain.shape[0]
    if (
        kv_heads == GROUPS
        and GROUPS * n_x == n_ep
        and n_x == 2
        and expert_ids.shape[1] == n_x
        and w_gate.shape[0] == 1
        and lax.axis_size("tp") == 4
        and query_rows.shape[0] % GRID == 0
    ):
        return layer(
            n_x,
            query_rows,
            key_rows,
            value_rows,
            query_gain,
            key_gain,
            w_out,
            mixer_gain,
            expert_input,
            expert_ids,
            expert_weights,
            input_gain,
            w_gate,
            w_up,
            w_down,
            out_gain,
        )
    mixer_result = mixer_half(
        query_rows, key_rows, value_rows, query_gain, key_gain, w_out, mixer_gain
    )
    moe_result = expert_half(
        expert_input, expert_ids, expert_weights, input_gain, w_gate, w_up, w_down, out_gain
    )
    return (mixer_result, moe_result)


def solution(mesh):
    return jax.shard_map(
        per_device,
        mesh=mesh,
        in_specs=(
            P("ep", "tp"),
            P("ep", "tp"),
            P("ep", "tp"),
            P(),
            P(),
            P("tp", None),
            P(),
            P("ep", None),
            P("ep", None),
            P("ep", None),
            P(),
            P("ep", None, "tp"),
            P("ep", None, "tp"),
            P("ep", "tp", None),
            P("tp"),
        ),
        out_specs=(P(("ep", "tp"), None), P("ep", "tp")),
        check_vma=False,
    )
```

```python
import functools
import math

import jax
import jax.numpy as jnp
import numpy as np
from jax import lax
from jax.experimental import pallas as pl
from jax.experimental.pallas import tpu as pltpu
from jax.sharding import PartitionSpec as P

D = 2048
GRID = 64
GROUPS = 4
BLOCK_Q = 384
BLOCK_K = 768


EPS = 1e-06
THETA = 10000.0


def turn_half(half_part, position):
    half_width = half_part.shape[-1]
    frequency = THETA ** (-jnp.arange(0, half_width, 2, dtype=jnp.float32) / half_width)
    angles = position[:, None, None] * frequency[None, None, :]
    cosine = jnp.cos(angles)
    sine_part = jnp.sin(angles)
    first_half = half_part[..., : half_width // 2]
    second = half_part[..., half_width // 2 :]
    return jnp.concatenate(
        [first_half * cosine - second * sine_part, second * cosine + first_half * sine_part],
        axis=-1,
    )


def norm_turn(raw_rows, gain_vec, row_offset):
    row_count = raw_rows.shape[0]
    head_dim = gain_vec.shape[0]
    head_count = raw_rows.shape[1] // head_dim
    by_head = raw_rows.astype(jnp.float32).reshape(row_count, head_count, head_dim)
    scaled = (
        by_head * lax.rsqrt(jnp.mean(by_head * by_head, axis=-1, keepdims=True) + EPS) * gain_vec
    )
    position = row_offset + jnp.arange(row_count, dtype=jnp.int32)
    grid_row = (position // GRID).astype(jnp.float32)
    grid_col = (position % GRID).astype(jnp.float32)
    half_dim = head_dim // 2
    turned = jnp.concatenate(
        [turn_half(scaled[..., :half_dim], grid_row), turn_half(scaled[..., half_dim:], grid_col)],
        axis=-1,
    )
    return turned.reshape(row_count, head_count * head_dim).astype(jnp.bfloat16)


def attend_block(scale, block_keys, query, k_ref, k_cols, vt_ref):
    columns, head_dim = query.shape
    steps = k_ref.shape[0] // block_keys

    def step(index, carry):
        top, total, acc = carry
        rows = pl.ds(pl.multiple_of(index * block_keys, block_keys), block_keys)
        scores = (
            lax.dot_general(
                k_ref[rows, k_cols],
                query,
                (((1,), (1,)), ((), ())),
                preferred_element_type=jnp.float32,
            )
            * scale
        )
        new_top = jnp.maximum(top, jnp.max(scores, axis=0, keepdims=True))
        exponent = jnp.exp2(scores - new_top)
        factor = jnp.exp2(top - new_top)
        total = total * factor + jnp.sum(exponent, axis=0, keepdims=True)
        acc = acc * factor + jnp.dot(
            vt_ref[:, rows], exponent.astype(jnp.bfloat16), preferred_element_type=jnp.float32
        )
        return new_top, total, acc

    carry = (
        jnp.full((1, columns), -1e30, jnp.float32),
        jnp.zeros((1, columns), jnp.float32),
        jnp.zeros((head_dim, columns), jnp.float32),
    )
    if steps <= 8:
        for index in range(steps):
            carry = step(index, carry)
    else:
        carry = lax.fori_loop(0, steps, step, carry)
    _, total, acc = carry
    return (acc / total).T.astype(jnp.bfloat16)


def attend_kernel(scale, block_keys, q_ref, k_ref, v_ref, o_ref, vt_ref):
    @pl.when(pl.program_id(1) == 0)
    def _():
        vt_ref[...] = v_ref[...].T

    o_ref[...] = attend_block(scale, block_keys, q_ref[...], k_ref, slice(None), vt_ref)


def attend_send_kernel(
    n_ep, scale, block_keys, packed, out, vt_ref, stage, send_sem, recv_sem, own_sem
):
    me = lax.axis_index("ep")
    row_count = out.shape[0]
    head_dim = vt_ref.shape[0]
    barrier = pltpu.get_barrier_semaphore()
    for offset in range(1, n_ep):
        pl.semaphore_signal(
            barrier,
            inc=1,
            device_id={"ep": lax.rem(me + offset, n_ep)},
            device_id_type=pl.DeviceIdType.MESH,
        )
    pl.semaphore_wait(barrier, n_ep - 1)
    columns = pl.ds(pl.multiple_of(me * head_dim, head_dim), head_dim)

    def send(offset):
        return pltpu.make_async_remote_copy(
            src_ref=stage.at[offset - 1],
            dst_ref=out.at[:, columns],
            send_sem=send_sem.at[offset - 1],
            recv_sem=recv_sem.at[offset - 1],
            device_id={"ep": lax.rem(me + offset, n_ep)},
            device_id_type=pl.DeviceIdType.MESH,
        )

    vt_ref[...] = packed[:, 2 * head_dim : 3 * head_dim].T

    def block(index, carry):
        @pl.when(index > 0)
        def _():
            send(index).start()

        owner = lax.rem(me + index + 1, n_ep)
        rows = pl.ds(pl.multiple_of(owner * row_count, row_count), row_count)
        stage[index] = attend_block(
            scale,
            block_keys,
            packed[rows, 0:head_dim],
            packed,
            slice(head_dim, 2 * head_dim),
            vt_ref,
        )
        return carry

    lax.fori_loop(0, n_ep, block, 0)
    own = pltpu.make_async_copy(stage.at[n_ep - 1], out.at[:, columns], own_sem)
    own.start()
    for offset in range(1, n_ep):
        send(offset).wait()
    own.wait()


def attend_send(packed, n_ep, head_dim):
    tokens = packed.shape[0]
    row_count = tokens // n_ep
    return pl.pallas_call(
        functools.partial(
            attend_send_kernel,
            n_ep,
            head_dim**-0.5 * math.log2(math.e),
            divisor(tokens, BLOCK_K),
        ),
        in_specs=[pl.BlockSpec(memory_space=pltpu.VMEM)],
        out_specs=pl.BlockSpec(memory_space=pltpu.VMEM),
        out_shape=jax.ShapeDtypeStruct((row_count, n_ep * head_dim), jnp.bfloat16),
        scratch_shapes=[
            pltpu.VMEM((head_dim, tokens), jnp.bfloat16),
            pltpu.VMEM((n_ep, row_count, head_dim), jnp.bfloat16),
            pltpu.SemaphoreType.DMA((n_ep - 1,)),
            pltpu.SemaphoreType.DMA((n_ep - 1,)),
            pltpu.SemaphoreType.DMA,
        ],
        compiler_params=pltpu.CompilerParams(collective_id=0, has_side_effects=True),
        cost_estimate=pl.CostEstimate(
            flops=8 * tokens * tokens * head_dim,
            bytes_accessed=8 * tokens * head_dim,
            transcendentals=tokens * tokens,
        ),
        name="attend_send",
    )(packed)


def divisor(size, limit):
    block = limit
    while size % block:
        block -= 128
    return block


def attend(query, key, value, heads, head_dim, group_size, q_col, k_col, v_col):
    tokens = query.shape[0]
    keys = key.shape[0]
    block_q = divisor(tokens, BLOCK_Q)
    block_k = divisor(keys, BLOCK_K)
    flops = 4 * heads * tokens * keys * head_dim
    return pl.pallas_call(
        functools.partial(attend_kernel, head_dim**-0.5 * math.log2(math.e), block_k),
        grid=(heads, tokens // block_q),
        in_specs=[
            pl.BlockSpec((block_q, head_dim), lambda h, i: (i, q_col + h)),
            pl.BlockSpec((keys, head_dim), lambda h, i: (0, k_col + h // group_size)),
            pl.BlockSpec((keys, head_dim), lambda h, i: (0, v_col + h // group_size)),
        ],
        out_specs=pl.BlockSpec((block_q, head_dim), lambda h, i: (i, h)),
        out_shape=jax.ShapeDtypeStruct((tokens, heads * head_dim), jnp.bfloat16),
        scratch_shapes=[pltpu.VMEM((head_dim, keys), jnp.bfloat16)],
        compiler_params=pltpu.CompilerParams(dimension_semantics=("arbitrary", "arbitrary")),
        cost_estimate=pl.CostEstimate(
            flops=2 * flops,
            bytes_accessed=8 * tokens * heads * head_dim,
            transcendentals=heads * tokens * keys,
        ),
        name="attend",
    )(query, key, value)


def mixer_half(query_rows, key_rows, value_rows, query_gain, key_gain, w_out, mixer_gain):
    row_count = query_rows.shape[0]
    head_dim = query_gain.shape[0]
    n_ep = lax.axis_size("ep")
    row_offset = lax.axis_index("ep") * row_count
    query_turned = norm_turn(query_rows, query_gain, row_offset)
    key_turned = norm_turn(key_rows, key_gain, row_offset)
    local_heads = query_rows.shape[1] // head_dim
    group_size = query_rows.shape[1] // key_rows.shape[1]
    if local_heads == n_ep:
        by_head = [
            x.reshape(row_count, -1, head_dim).transpose(1, 0, 2)
            for x in (query_turned, key_turned, value_rows)
        ]
        outgoing = jnp.concatenate(
            [by_head[0]] + [jnp.repeat(x, group_size, axis=0) for x in by_head[1:]], axis=2
        )
        arrived = lax.all_to_all(outgoing, "ep", split_axis=0, concat_axis=0, tiled=True)
        packed = arrived.reshape(n_ep * row_count, 3 * head_dim)
        attended = attend_send(packed, n_ep, head_dim)
    else:
        key_all = lax.all_gather(key_turned, "ep", axis=0, tiled=True)
        value_all = lax.all_gather(value_rows, "ep", axis=0, tiled=True)
        attended = attend(
            query_turned, key_all, value_all, local_heads, head_dim, group_size, 0, 0, 0
        )
    mixed_sum = lax.psum_scatter(
        jnp.dot(attended, w_out, preferred_element_type=jnp.float32).astype(jnp.bfloat16),
        "tp",
        scatter_dimension=0,
        tiled=True,
    ).astype(jnp.float32)
    scaled = (
        mixed_sum
        * lax.rsqrt(jnp.mean(mixed_sum * mixed_sum, axis=1, keepdims=True) + EPS)
        * mixer_gain
    )
    return scaled.astype(jnp.bfloat16)


def expert_half(
    expert_input, expert_ids, expert_weights, input_gain, w_gate, w_up, w_down, out_gain
):
    row_count, width = expert_input.shape
    top_count = expert_ids.shape[1]
    n_tp = lax.axis_size("tp")
    expert_total = w_gate.shape[0] * lax.axis_size("ep")
    inner_count = expert_total // GROUPS
    capacity = 3 * row_count // (4 * inner_count)
    slots = expert_total * capacity
    inputs_f = expert_input.astype(jnp.float32)
    normed = (
        inputs_f
        * lax.rsqrt(jnp.mean(inputs_f * inputs_f, axis=1, keepdims=True) + EPS)
        * input_gain
    ).astype(jnp.bfloat16)
    row_index = jnp.arange(row_count, dtype=jnp.int32)
    before = row_index[None, :] < row_index[:, None]
    slot_index = jnp.arange(slots, dtype=jnp.int32)
    slot_of = []
    for k in range(top_count):
        same = jnp.zeros((row_count, row_count), bool)
        for other in range(top_count):
            same = same | (expert_ids[:, k][:, None] == expert_ids[:, other][None, :])
        rank = jnp.sum((same & before).astype(jnp.int32), axis=1)
        slot_of.append(expert_ids[:, k] * capacity + rank)
    chosen = [slot_index[:, None] == slot[None, :] for slot in slot_of]
    picker = functools.reduce(jnp.logical_or, chosen).astype(jnp.bfloat16)
    share = width // n_tp
    own = lax.dynamic_slice_in_dim(normed, lax.axis_index("tp") * share, share, axis=1)
    outgoing = jnp.dot(picker, own, preferred_element_type=jnp.float32).astype(jnp.bfloat16)
    arrived = lax.all_to_all(
        outgoing.reshape(expert_total, capacity, share),
        "ep",
        split_axis=0,
        concat_axis=0,
        tiled=True,
    ).reshape(slots, share)
    shares = lax.all_gather(arrived, "tp", axis=0, tiled=False)
    arrived = jnp.concatenate([shares[j] for j in range(n_tp)], axis=1)
    gate_pre = jnp.dot(arrived, w_gate[0], preferred_element_type=jnp.float32)
    up_pre = jnp.dot(arrived, w_up[0], preferred_element_type=jnp.float32)
    hidden = (jax.nn.silu(gate_pre) * up_pre).astype(jnp.bfloat16)
    partial_term = jnp.dot(hidden, w_down[0], preferred_element_type=jnp.float32)
    summed = lax.psum_scatter(
        partial_term.astype(jnp.bfloat16), "tp", scatter_dimension=1, tiled=True
    )
    returned = lax.all_to_all(summed, "ep", split_axis=0, concat_axis=0, tiled=True)
    combined = jnp.zeros((row_count, returned.shape[1]), jnp.float32)
    for k in range(top_count):
        select = (slot_of[k][:, None] == slot_index[None, :]).astype(jnp.bfloat16)
        picked = jnp.dot(select, returned, preferred_element_type=jnp.float32)
        combined = combined + picked * expert_weights[:, k][:, None]
    squares = lax.psum(jnp.sum(combined * combined, axis=1), "tp")
    scaled = combined * lax.rsqrt(squares / D + EPS)[:, None] * out_gain
    return scaled.astype(jnp.bfloat16)


MESH_ID = pl.DeviceIdType.MESH
FF_STEP = 256


def remote(src, dst, send_sem, recv_sem, ep, tp):
    return pltpu.make_async_remote_copy(
        src_ref=src,
        dst_ref=dst,
        send_sem=send_sem,
        recv_sem=recv_sem,
        device_id={"ep": ep, "tp": tp},
        device_id_type=MESH_ID,
    )


def aligned(index, size):
    return pl.ds(pl.multiple_of(index * size, size), size)


def turn_rows(raw, gain, cosine, sine, low_lane):
    rows = raw.astype(jnp.float32)
    mean = jnp.mean(rows * rows, axis=1, keepdims=True)
    rows = rows * lax.rsqrt(mean + EPS) * gain
    head_dim = rows.shape[1]
    quarter = head_dim // 4
    swapped = jnp.where(
        low_lane, pltpu.roll(rows, head_dim - quarter, 1), pltpu.roll(rows, quarter, 1)
    )
    return (rows * cosine + swapped * sine).astype(jnp.bfloat16)


def attend_keys(query, keys, values_t, state):
    top, total, acc = state
    scores = lax.dot_general(
        keys, query, (((1,), (1,)), ((), ())), preferred_element_type=jnp.float32
    )
    new_top = jnp.maximum(top, jnp.max(scores, axis=0, keepdims=True))
    exponent = jnp.exp2(scores - new_top)
    factor = jnp.exp2(top - new_top)
    total = total * factor + jnp.sum(exponent, axis=0, keepdims=True)
    acc = acc * factor + jnp.dot(
        values_t, exponent.astype(jnp.bfloat16), preferred_element_type=jnp.float32
    )
    return new_top, total, acc


def load_inputs(n_ep, n_x, n_tp, cap, count, *refs):
    held, weights, outs = refs[:count], refs[count : count + 4], refs[count + 4 : count + 6]
    loaded, sems, rest = refs[count + 6 : 2 * count + 6], refs[2 * count + 6], refs[2 * count + 7 :]
    loads = [pltpu.make_async_copy(held[i], loaded[i], sems.at[i]) for i in range(count)]
    for i in (8, 9, 10, 11, 1, 6, 3, 4, 2, 0, 5, 7, 12):
        loads[i].start()
    layer_kernel(n_ep, n_x, n_tp, cap, loads, *loaded, *weights, *outs, *rest)


def layer_kernel(
    n_ep,
    n_x,
    n_tp,
    cap,
    loads,
    q_ref,
    k_ref,
    v_ref,
    row_table,
    col_table,
    q_gain,
    k_gain,
    mixer_gain,
    x_ref,
    ids_ref,
    weight_ref,
    in_gain,
    out_gain,
    w_gate,
    w_up,
    w_down,
    w_out,
    mixer_out,
    moe_out,
    wg,
    wu,
    wd,
    wo,
    q_stage,
    k_stage,
    v_stage,
    k_all,
    vt_all,
    q_all,
    tops,
    totals,
    accs,
    o_stage,
    o_all,
    picker,
    x_stage,
    x_all,
    mix_stage,
    mix_all,
    hidden,
    part_send,
    part_keep,
    part_recv,
    pair_send,
    pair_recv,
    rows_out,
    rows_in,
    joined,
    returned,
    squares_send,
    squares_recv,
    head_part,
    head_recv,
    head_pair,
    head_last,
    w_sem,
    own_sem,
    mz_s,
    mz_r,
    mw_s,
    mw_r,
    mx_s,
    mx_r,
    my_s,
    my_r,
    mc_s,
    mc_r,
    k_s,
    k_r,
    v_s,
    v_r,
    kf_s,
    kf_r,
    vf_s,
    vf_r,
    q_s,
    q_r,
    o_s,
    o_r,
    pc_s,
    pc_r,
    py_s,
    py_r,
    jx_s,
    jx_r,
    ret_s,
    ret_r,
    sq_s,
    sq_r,
    hc_s,
    hc_r,
    hy_s,
    hy_r,
):
    me = lax.axis_index("ep")
    t = lax.axis_index("tp")
    n_z = n_ep // n_x
    slots = n_z
    planes = slots // n_x
    z = me // n_x
    x = lax.rem(me, n_x)
    other_x = 1 - x
    core = t + 1 - 2 * lax.rem(t, 2)
    across = lax.rem(t + 2, n_tp)
    diagonal = lax.rem(core + 2, n_tp)
    x_peer = z * n_x + other_x
    block = me // slots
    slot = lax.rem(me, slots)
    level = slot // n_x
    far = level + (1 - block) - 2 * level * (1 - block)

    def plane(offset):
        return lax.rem(z + offset, n_z)

    def source(offset):
        return lax.rem(z + n_z - offset, n_z)

    def peer(index):
        flip_level = lax.rem(index + 1, 2) * (1 - index // 3)
        flip_x = lax.rem((index + 1) // 2, 2)
        to_level = level + flip_level - 2 * level * flip_level
        to_x = x + flip_x - 2 * x * flip_x
        return to_level * n_x + to_x

    sent = []

    def go(copy):
        copy.start()
        sent.append(copy)
        return copy

    weights = [
        pltpu.make_async_copy(w_gate.at[0], wg, w_sem.at[0]),
        pltpu.make_async_copy(w_up.at[0], wu, w_sem.at[1]),
        pltpu.make_async_copy(w_down.at[0], wd, w_sem.at[2]),
        pltpu.make_async_copy(w_out, wo, w_sem.at[3]),
    ]

    barrier = pltpu.get_barrier_semaphore()
    greeted = [(plane(o) * n_x + x, t) for o in range(1, n_z)]
    greeted += [(block * slots + peer(i), t) for i in (1, 2)]
    greeted += [((1 - block) * slots + peer(i), t) for i in (1, 2)]
    greeted += [(me, core), (me, across), (me, diagonal)]
    for ep, tp in greeted:
        pl.semaphore_signal(barrier, inc=1, device_id={"ep": ep, "tp": tp}, device_id_type=MESH_ID)

    for i in (8, 9, 10, 11):
        loads[i].wait()

    for copy in weights:
        copy.start()

    rows, width = x_ref.shape
    share = width // n_tp
    own_cols = aligned(t, share)
    group_rows = n_z * cap
    x_full = x_ref[...].astype(jnp.float32)
    scale = lax.rsqrt(jnp.mean(x_full * x_full, axis=1, keepdims=True) + EPS)
    normed = (x_ref[:, own_cols].astype(jnp.float32) * scale * in_gain[:, own_cols]).astype(
        jnp.bfloat16
    )
    id_rows = ids_ref[...]
    first_id = jnp.broadcast_to(id_rows[0:1, :].astype(jnp.float32), (128, rows)).T
    lane = lax.broadcasted_iota(jnp.int32, (rows, 128), 1).astype(jnp.float32)
    in_group = (first_id >= lane * n_x) & (first_id < lane * n_x + n_x)
    row_at = lax.broadcasted_iota(jnp.int32, (rows, rows), 0)
    col_at = lax.broadcasted_iota(jnp.int32, (rows, rows), 1)
    earlier = jnp.where(col_at < row_at, 1.0, 0.0).astype(jnp.bfloat16)
    counts = jnp.dot(
        earlier,
        jnp.where(in_group, 1.0, 0.0).astype(jnp.bfloat16),
        preferred_element_type=jnp.float32,
    )
    place = jnp.sum(jnp.where(in_group, counts + lane * cap, 0.0), axis=1, keepdims=True)
    place_at = lax.broadcasted_iota(jnp.int32, (rows, group_rows), 1).astype(jnp.float32)
    picks = jnp.where(place_at == place, 1.0, 0.0)
    picker[...] = picks.astype(jnp.bfloat16)
    x_stage[...] = lax.dot_general(
        picker[...], normed, (((0,), (0,)), ((), ())), preferred_element_type=jnp.float32
    ).astype(jnp.bfloat16)
    odd = lax.rem(id_rows, n_x) == 1
    mix = weight_ref[...]
    second = jnp.sum(jnp.where(odd, mix, 0.0), axis=0, keepdims=True)
    first = jnp.sum(jnp.where(odd, 0.0, mix), axis=0, keepdims=True)
    at_row = lax.broadcasted_iota(jnp.int32, (8, rows), 0)
    both = jnp.where(at_row == 0, first, jnp.where(at_row == 1, second, 0.0))
    placed = jnp.dot(
        both, picks, preferred_element_type=jnp.float32, precision=lax.Precision.HIGHEST
    )
    for g in range(n_z):
        mix_stage[g, :, 0:cap] = placed[:, g * cap : (g + 1) * cap]

    for i in (1, 2, 3, 4, 6):
        loads[i].wait()
    tokens = k_ref.shape[0]
    head_dim = q_gain.shape[1]
    heads = q_ref.shape[1] // (slots * head_dim)
    own_tokens = tokens // n_tp
    half_own = own_tokens // 2
    half_tokens = tokens // 2
    lanes = lax.broadcasted_iota(jnp.int32, (tokens, head_dim), 1)
    low_lane = lax.rem(lanes, head_dim // 2) < head_dim // 4
    grid_rows = tokens // GRID
    by_row = lax.broadcasted_iota(jnp.int32, (GRID, head_dim), 1) < head_dim // 2

    def table(which):
        return jnp.concatenate(
            [
                jnp.where(
                    by_row, row_table[which, pl.ds(me * grid_rows + r, 1), :], col_table[which]
                )
                for r in range(grid_rows)
            ],
            axis=0,
        )

    cosine, sine = table(0), table(1)
    for g in range(slots):
        cols = slice(g * head_dim, (g + 1) * head_dim)
        k_stage[g] = turn_rows(k_ref[:, cols], k_gain[...], cosine, sine, low_lane)
        v_stage[g] = v_ref[:, cols].T
    pl.semaphore_wait(barrier, len(greeted))

    def chunk_at(region, index):
        return x_all.at[region, aligned(index, cap), own_cols]

    own_rows = x_stage.at[aligned(z, cap), :]
    moe_z = []
    for o in (2, 1, 3):
        to = plane(o)
        moe_z.append(
            go(
                remote(
                    x_stage.at[aligned(to, cap), :],
                    chunk_at(0, z),
                    mz_s.at[o - 1],
                    mz_r.at[o - 1],
                    to * n_x + x,
                    t,
                )
            )
        )
    moe_w = []
    for o in (2, 1, 3):
        to = plane(o)
        moe_w.append(
            go(
                remote(
                    mix_stage.at[to], mix_all.at[z], mw_s.at[o - 1], mw_r.at[o - 1], to * n_x + x, t
                )
            )
        )
    own_x = pltpu.make_async_copy(own_rows, chunk_at(0, z), own_sem.at[0])
    own_x.start()
    own_mix = pltpu.make_async_copy(mix_stage.at[z], mix_all.at[z], own_sem.at[1])
    own_mix.start()
    moe_y = [[go(remote(own_rows, chunk_at(0, z), my_s.at[0, 0], my_r.at[0, 0], me, across))], []]
    moe_x = [go(remote(own_rows, chunk_at(1, z), mx_s.at[0], mx_r.at[0], x_peer, t))]

    def k_at(index):
        return k_all.at[aligned(index, tokens), :]

    def v_at(index):
        return vt_all.at[:, aligned(index, tokens)]

    def near_keys(i, index):
        to = peer(i)
        ep = block * slots + to
        return (
            go(remote(k_stage.at[to], k_at(index), k_s.at[i], k_r.at[i], ep, t)),
            go(remote(v_stage.at[to], v_at(index), v_s.at[i], v_r.at[i], ep, t)),
        )

    def near_queries(i):
        to = peer(i)
        ep = block * slots + to
        go(remote(q_stage.at[to], q_all.at[slot], q_s.at[i], q_r.at[i], ep, t))

    straight_keys = near_keys(0, 1)

    for i in (0, 5, 7, 12):
        loads[i].wait()
    to_exponent = head_dim**-0.5 * math.log2(math.e)
    for g in range(slots):
        for h in range(heads):
            cols = slice((g * heads + h) * head_dim, (g * heads + h + 1) * head_dim)
            turned = turn_rows(q_ref[:, cols], q_gain[...] * to_exponent, cosine, sine, low_lane)
            for part in range(2):
                for owner in range(n_tp):
                    first_row = h * tokens + part * half_tokens + owner * half_own
                    from_row = owner * own_tokens + part * half_own
                    q_stage[g, first_row : first_row + half_own, :] = turned[
                        from_row : from_row + half_own
                    ]
    own_copies = [
        pltpu.make_async_copy(k_stage.at[slot], k_at(0), own_sem.at[2]),
        pltpu.make_async_copy(v_stage.at[slot], v_at(0), own_sem.at[3]),
        pltpu.make_async_copy(q_stage.at[slot], q_all.at[slot], own_sem.at[4]),
    ]
    for copy in own_copies:
        copy.start()

    for copy, o in zip(moe_z, (2, 1, 3)):
        copy.wait_recv()
        here = chunk_at(0, source(o))
        moe_y[0].append(go(remote(here, here, my_s.at[0, o], my_r.at[0, o], me, across)))
        moe_x.append(go(remote(here, chunk_at(1, source(o)), mx_s.at[o], mx_r.at[o], x_peer, t)))
    own_x.wait()

    near_queries(0)

    def far_copies(order, cross):
        flip = 1 - order - far + 2 * order * far
        to_level = level + flip - 2 * level * flip
        to = to_level * n_x + (other_x if cross else x)
        ep = (1 - block) * slots + to
        at = planes * (1 + 2 * cross) + far
        send, arrive = planes * cross + order, planes * cross + far
        return (
            remote(k_stage.at[to], k_at(at), kf_s.at[send], kf_r.at[arrive], ep, t),
            remote(v_stage.at[to], v_at(at), vf_s.at[send], vf_r.at[arrive], ep, t),
        )

    def send_far(cross):
        for order in range(planes):
            for copy in far_copies(order, cross):
                copy.start()

    def wait_far(cross, orders):
        for order in orders:
            at, arrive = planes * (1 + 2 * cross) + order, planes * cross + order
            remote(
                k_stage.at[slot], k_at(at), kf_s.at[0], kf_r.at[arrive], me, core
            ).wait_recv()
            remote(
                v_stage.at[slot], v_at(at), vf_s.at[0], vf_r.at[arrive], me, core
            ).wait_recv()

    send_far(0)
    near_queries(1)
    near_queries(2)

    def cols_at(region, tp):
        return x_all.at[region, :, aligned(tp, share)]

    def to_core(region, index, tp):
        return go(
            remote(
                cols_at(region, tp),
                cols_at(region, tp),
                mc_s.at[region, index],
                mc_r.at[region, index],
                me,
                core,
            )
        )

    moe_c = [[to_core(0, 0, t)], []]
    for copy, o in zip(moe_x, (0, 2, 1, 3)):
        copy.wait_recv()
        here = chunk_at(1, source(o))
        moe_y[1].append(go(remote(here, here, my_s.at[1, o], my_r.at[1, o], me, across)))
    moe_c[1].append(to_core(1, 0, t))
    crossed_keys = near_keys(1, slots) + near_keys(2, slots + 1)
    send_far(1)
    for copy in moe_y[0]:
        copy.wait_recv()
    moe_c[0].append(to_core(0, 1, across))

    blocks = (core, diagonal, t, across)
    inner_width = wg.shape[1]

    def part_copy(region, index):
        return remote(
            part_send.at[region, index],
            part_recv.at[region, index],
            pc_s.at[region, index],
            pc_r.at[region, index],
            me,
            core,
        )

    def experts(region):
        for copy in moe_c[region]:
            copy.wait_recv()
        if region == 0:
            weights[0].wait()
            weights[1].wait()

        def pre(index, carry):
            cols = aligned(index, FF_STEP)
            rows_now = x_all[region]
            gate = jnp.dot(rows_now, wg[:, cols], preferred_element_type=jnp.float32)
            up = jnp.dot(rows_now, wu[:, cols], preferred_element_type=jnp.float32)
            hidden[:, cols] = (gate / (1.0 + jnp.exp(-gate)) * up).astype(jnp.bfloat16)
            return carry

        lax.fori_loop(0, inner_width // FF_STEP, pre, 0)
        if region == 0:
            weights[2].wait()
        for index in (1, 0, 3, 2):
            part = jnp.dot(
                hidden[...],
                wd[:, aligned(blocks[index], share)],
                preferred_element_type=jnp.float32,
            ).astype(jnp.bfloat16)
            if index < 2:
                part_send[region, index] = part
                go(part_copy(region, index))
            else:
                part_keep[region, index - 2] = part

    def pair_copy(region):
        return remote(
            pair_send.at[region], pair_recv.at[region], py_s.at[region], py_r.at[region], me, across
        )

    def pair(region):
        part_copy(region, 1).wait_recv()
        pair_send[region] = (
            part_keep[region, 1].astype(jnp.float32) + part_recv[region, 1].astype(jnp.float32)
        ).astype(jnp.bfloat16)
        pair_copy(region).start()

    experts(0)
    step = 2 * tokens
    queries = heads * tokens

    def key_step(index):
        return slice(index * step, (index + 1) * step)

    def load_state(to):
        return tops[to, 0:1, :], totals[to, 0:1, :], accs[to]

    def save_state(to, state):
        tops[to, 0:1, :], totals[to, 0:1, :], accs[to] = state

    def own_block(turn, carry):
        index = lax.rem(turn + slots - 1, slots)
        to = peer(index)

        @pl.when(index < slots - 1)
        def _():
            remote(
                q_stage.at[to], q_all.at[to], q_s.at[index], q_r.at[index], me, core
            ).wait_recv()

        state = (
            jnp.full((1, queries), -1e30, jnp.float32),
            jnp.zeros((1, queries), jnp.float32),
            jnp.zeros((head_dim, queries), jnp.float32),
        )
        for s in range(slots // 2):
            state = attend_keys(q_all[to], k_all[key_step(s), :], vt_all[:, key_step(s)], state)
        save_state(to, state)

        @pl.when(turn == 0)
        def _():
            pair(1)

        return carry

    for copy in moe_y[1]:
        copy.wait_recv()
    moe_c[1].append(to_core(1, 1, across))
    pair(0)
    experts(1)
    for copy in own_copies:
        copy.wait()
    for copy in straight_keys:
        copy.wait_recv()
    wait_far(0, range(planes))
    lax.fori_loop(0, slots, own_block, 0)

    join = remote(rows_out.at[1], rows_in, jx_s.at[0], jx_r.at[0], x_peer, t)
    sent.append(join)

    def expert_rows():
        for region in (1, 0):
            part_copy(region, 0).wait_recv()
            pair_copy(region).wait_recv()
            rows_out[region] = (
                part_keep[region, 0].astype(jnp.float32)
                + part_recv[region, 0].astype(jnp.float32)
                + pair_recv[region].astype(jnp.float32)
            ).astype(jnp.bfloat16)
            if region == 1:
                join.start()

    for copy in crossed_keys:
        copy.wait_recv()

    def near_block(index, carry):
        to = peer(index)
        s = slots // 2
        save_state(
            to,
            attend_keys(q_all[to], k_all[key_step(s), :], vt_all[:, key_step(s)], load_state(to)),
        )
        @pl.when(index == 0)
        def _():
            expert_rows()

        return carry

    lax.fori_loop(0, slots, near_block, 0)

    def output_copy(index, part):
        to = peer(index)
        at = slice(part * half_tokens, (part + 1) * half_tokens)
        return remote(
            o_stage.at[to, :, at, :],
            o_all.at[pl.ds(slot * heads, heads), at, :],
            o_s.at[part, index],
            o_r.at[part, index],
            block * slots + to,
            t,
        )

    def last_block(turn, carry):
        index = lax.rem(2 * slots - 2 - turn, slots)
        to = peer(index)
        at = keys_of(2 * slots - 1)
        _, total, acc = attend_keys(
            q_all[to], k_all[at, :], vt_all[:, at], load_state(to)
        )
        out = (acc / total).T.astype(jnp.bfloat16)
        for h in range(heads):
            o_stage[to, h] = out[h * tokens : (h + 1) * tokens]

        @pl.when(turn == 0)
        def _():
            output_copy(2, 0).start()

        @pl.when(turn == 1)
        def _():
            output_copy(1, 0).start()

        @pl.when(turn == 2)
        def _():
            output_copy(0, 0).start()
            for i in (2, 0, 1):
                output_copy(i, 1).start()

        return carry

    wait_far(1, (0,))

    def keys_of(index):
        return slice(index * tokens, (index + 1) * tokens)

    def next_block(index, carry):
        to = peer(index)
        at = keys_of(2 * slots - 2)
        save_state(to, attend_keys(q_all[to], k_all[at, :], vt_all[:, at], load_state(to)))
        return carry

    lax.fori_loop(0, slots, next_block, 0)
    wait_far(1, (1,))
    lax.fori_loop(0, slots, last_block, 0)
    own_o = pltpu.make_async_copy(
        o_stage.at[slot], o_all.at[pl.ds(slot * heads, heads)], own_sem.at[6]
    )
    own_o.start()

    weights[3].wait()
    own_o.wait()

    out_width = wo.shape[1]
    all_heads = slots * heads

    pieces = 2
    piece_width = out_width // pieces

    def project(part):
        at = slice(part * half_tokens, (part + 1) * half_tokens)
        taken = jnp.concatenate([o_all[h, at, :] for h in range(all_heads)], axis=1)
        copies = []
        for piece in range(pieces):

            def columns(index, carry):
                cols = aligned(index, 512)
                out = jnp.dot(taken, wo[:, cols], preferred_element_type=jnp.float32).astype(
                    jnp.bfloat16
                )
                for owner in range(n_tp):
                    head_part[part, owner, :, cols] = out[owner * half_own : (owner + 1) * half_own]
                return carry

            lax.fori_loop(
                piece * piece_width // 512, (piece + 1) * piece_width // 512, columns, 0
            )
            cols = slice(piece * piece_width, (piece + 1) * piece_width)
            copies.append(
                [
                    go(
                        remote(
                            head_part.at[part, to, :, cols],
                            head_recv.at[part, i, :, cols],
                            hc_s.at[part, piece, i],
                            hc_r.at[part, piece, i],
                            me,
                            core,
                        )
                    )
                    for i, to in ((1, diagonal), (0, core))
                ]
            )
        return copies

    def to_across(part, copies):
        sums = []
        for piece in range(pieces):
            cols = slice(piece * piece_width, (piece + 1) * piece_width)
            copies[piece][0].wait_recv()
            head_pair[part, :, cols] = (
                head_part[part, across, :, cols].astype(jnp.float32)
                + head_recv[part, 1, :, cols].astype(jnp.float32)
            ).astype(jnp.bfloat16)
            sums.append(
                go(
                    remote(
                        head_pair.at[part, :, cols],
                        head_last.at[part, :, cols],
                        hy_s.at[part, piece],
                        hy_r.at[part, piece],
                        me,
                        across,
                    )
                )
            )
        return sums

    for i in (0, 1, 2):
        output_copy(i, 0).wait_recv()
    first_half = project(0)
    first_y = to_across(0, first_half)
    for copy in moe_w:
        copy.wait_recv()
    own_mix.wait()
    join.wait_recv()
    mine_first = x == 0
    for g in range(n_z):
        mix_cols = mix_all[g].T
        here = slice(g * cap, (g + 1) * cap)
        mine = rows_out[0, here, :].astype(jnp.float32)
        theirs = rows_in[here, :].astype(jnp.float32)
        first_w, second_w = mix_cols[0:cap, 0:1], mix_cols[0:cap, 1:2]
        joined[here, :] = (
            mine * jnp.where(mine_first, first_w, second_w)
            + theirs * jnp.where(mine_first, second_w, first_w)
        ).astype(jnp.bfloat16)

    def back_at():
        return returned.at[aligned(z, cap), :]

    own_return = pltpu.make_async_copy(joined.at[aligned(z, cap), :], back_at(), own_sem.at[5])
    own_return.start()
    returns = []
    for o in (2, 1, 3):
        to = plane(o)
        returns.append(
            go(
                remote(
                    joined.at[aligned(to, cap), :],
                    back_at(),
                    ret_s.at[o - 1],
                    ret_r.at[o - 1],
                    to * n_x + x,
                    t,
                )
            )
        )
    for i in (0, 1, 2):
        output_copy(i, 1).wait_recv()
    second_half = project(1)
    second_y = to_across(1, second_half)
    for copy in returns:
        copy.wait_recv()
    own_return.wait()
    combined = jnp.dot(picker[...], returned[...], preferred_element_type=jnp.float32)
    squares = jnp.sum(combined * combined, axis=1, keepdims=True)
    squares_send[...] = jnp.broadcast_to(squares, (rows, 128)).T[0:8, :]
    square_copies = [
        go(remote(squares_send, squares_recv.at[i], sq_s.at[i], sq_r.at[i], me, tp))
        for i, tp in enumerate((core, across, diagonal))
    ]

    for copy in square_copies:
        copy.wait_recv()
    all_squares = squares_send[...] + squares_recv[0] + squares_recv[1] + squares_recv[2]
    spread = jnp.broadcast_to(all_squares[0:1, :], (128, rows)).T[:, 0:1]
    moe_out[...] = (combined * lax.rsqrt(spread / width + EPS) * out_gain[...]).astype(
        jnp.bfloat16
    )

    for part, copies, last in ((0, first_half, first_y), (1, second_half, second_y)):
        for piece in range(pieces):
            copies[piece][1].wait_recv()
            last[piece].wait_recv()
        mixed = (
            head_part[part, t].astype(jnp.float32)
            + head_recv[part, 0].astype(jnp.float32)
            + head_last[part].astype(jnp.float32)
        )
        mean = jnp.mean(mixed * mixed, axis=1, keepdims=True)
        mixer_out[part * half_own : (part + 1) * half_own, :] = (
            mixed * lax.rsqrt(mean + EPS) * mixer_gain[...]
        ).astype(jnp.bfloat16)

    for copy in sent:
        copy.wait_send()
    for region in range(n_x):
        pair_copy(region).wait_send()
    for cross in range(n_x):
        for order in range(planes):
            for copy in far_copies(order, cross):
                copy.wait_send()
    for i in (0, 1, 2):
        for part in range(2):
            output_copy(i, part).wait_send()


def hand_over(mixer_in, moe_in, mixer_out, moe_out):
    mixer_out[...] = mixer_in[...]
    moe_out[...] = moe_in[...]


def turn_tables(row_count, head_dim):
    half_width = head_dim // 2
    steps = np.arange(0, half_width, 2, dtype=np.float32) / np.float32(half_width)
    frequency = np.float32(THETA) ** -steps
    sign = np.where(np.arange(half_width) < half_width // 2, -1.0, 1.0)
    tables = []
    for count in (row_count, GRID):
        angles = np.arange(count, dtype=np.float32)[:, None] * frequency[None, :]
        angles = np.tile(angles, (1, 2)).astype(np.float64)
        both = np.stack([np.cos(angles), np.sin(angles) * sign])
        tables.append(np.tile(both, (1, 1, 2)).astype(np.float32))
    return tables


def layer(
    n_x,
    query_rows,
    key_rows,
    value_rows,
    query_gain,
    key_gain,
    w_out,
    mixer_gain,
    expert_input,
    expert_ids,
    expert_weights,
    input_gain,
    w_gate,
    w_up,
    w_down,
    out_gain,
):
    n_ep = lax.axis_size("ep")
    n_tp = lax.axis_size("tp")
    n_z = n_ep // n_x
    slots = n_z
    tokens = query_rows.shape[0]
    head_dim = query_gain.shape[0]
    heads = query_rows.shape[1] // (slots * head_dim)
    rows, width = expert_input.shape
    share = width // n_tp
    inner = w_gate.shape[2]
    cap = -(-(3 * rows // (4 * n_x)) // 16) * 16
    row_table, col_table = turn_tables(n_ep * tokens // GRID, head_dim)
    bf16, f32 = jnp.bfloat16, jnp.float32
    vmem = pl.BlockSpec(memory_space=pltpu.VMEM)
    hbm = pl.BlockSpec(memory_space=pltpu.HBM)
    dma = pltpu.SemaphoreType.DMA
    group_rows = n_z * cap
    own_tokens = tokens // n_tp
    half_own = own_tokens // 2
    queries = heads * tokens
    keys = n_ep * tokens
    inputs = (
        query_rows,
        key_rows,
        value_rows,
        jnp.asarray(row_table),
        jnp.asarray(col_table),
        query_gain[None, :],
        key_gain[None, :],
        mixer_gain[None, :],
        expert_input,
        expert_ids.T,
        expert_weights.T,
        input_gain[None, :],
        out_gain[None, :],
    )
    scratch = [pltpu.VMEM(value.shape, value.dtype) for value in inputs]
    scratch += [
        dma((len(inputs),)),
        pltpu.VMEM(w_gate.shape[1:], bf16),
        pltpu.VMEM(w_up.shape[1:], bf16),
        pltpu.VMEM(w_down.shape[1:], bf16),
        pltpu.VMEM(w_out.shape, bf16),
        pltpu.VMEM((slots, queries, head_dim), bf16),
        pltpu.VMEM((slots, tokens, head_dim), bf16),
        pltpu.VMEM((slots, head_dim, tokens), bf16),
        pltpu.VMEM((keys, head_dim), bf16),
        pltpu.VMEM((head_dim, keys), bf16),
        pltpu.VMEM((slots, queries, head_dim), bf16),
        pltpu.VMEM((slots, 8, queries), f32),
        pltpu.VMEM((slots, 8, queries), f32),
        pltpu.VMEM((slots, head_dim, queries), f32),
        pltpu.VMEM((slots, heads, tokens, head_dim), bf16),
        pltpu.VMEM((slots * heads, tokens, head_dim), bf16),
        pltpu.VMEM((rows, group_rows), bf16),
        pltpu.VMEM((group_rows, share), bf16),
        pltpu.VMEM((n_x, group_rows, width), bf16),
        pltpu.VMEM((n_z, 8, 128), f32),
        pltpu.VMEM((n_z, 8, 128), f32),
        pltpu.VMEM((group_rows, inner), bf16),
        pltpu.VMEM((n_x, 2, group_rows, share), bf16),
        pltpu.VMEM((n_x, 2, group_rows, share), bf16),
        pltpu.VMEM((n_x, 2, group_rows, share), bf16),
        pltpu.VMEM((n_x, group_rows, share), bf16),
        pltpu.VMEM((n_x, group_rows, share), bf16),
        pltpu.VMEM((n_x, group_rows, share), bf16),
        pltpu.VMEM((group_rows, share), bf16),
        pltpu.VMEM((group_rows, share), bf16),
        pltpu.VMEM((group_rows, share), bf16),
        pltpu.VMEM((8, rows), f32),
        pltpu.VMEM((3, 8, rows), f32),
        pltpu.VMEM((2, n_tp, half_own, width), bf16),
        pltpu.VMEM((2, 2, half_own, width), bf16),
        pltpu.VMEM((2, half_own, width), bf16),
        pltpu.VMEM((2, half_own, width), bf16),
        dma((4,)),
        dma((7,)),
    ]
    for shape in (
        (n_z - 1,),
        (n_z - 1,),
        (n_z,),
        (n_x, n_z),
        (n_x, 2),
        (slots - 1,),
        (slots - 1,),
        (slots,),
        (slots,),
        (slots - 1,),
        (2, slots - 1),
        (n_x, 2),
        (n_x,),
        (1,),
        (n_z - 1,),
        (3,),
        (2, 2, 2),
        (2, 2),
    ):
        scratch += [dma(shape), dma(shape)]
    mixer_rows, moe_rows = pl.pallas_call(
        functools.partial(load_inputs, n_ep, n_x, n_tp, cap, len(inputs)),
        in_specs=[hbm] * 17,
        out_specs=(vmem, vmem),
        out_shape=(
            jax.ShapeDtypeStruct((own_tokens, width), bf16),
            jax.ShapeDtypeStruct((rows, share), bf16),
        ),
        scratch_shapes=scratch,
        compiler_params=pltpu.CompilerParams(
            collective_id=0, has_side_effects=True, vmem_limit_bytes=62914560
        ),
        name="layer",
    )(
        *inputs,
        w_gate,
        w_up,
        w_down,
        w_out,
    )
    return pl.pallas_call(
        hand_over,
        in_specs=[vmem] * 2,
        out_specs=(vmem, vmem),
        out_shape=(
            jax.ShapeDtypeStruct(mixer_rows.shape, bf16),
            jax.ShapeDtypeStruct(moe_rows.shape, bf16),
        ),
        compiler_params=pltpu.CompilerParams(vmem_limit_bytes=4 * 1024 * 1024),
        name="hand_over",
    )(mixer_rows, moe_rows)


def per_device(
    query_rows,
    key_rows,
    value_rows,
    query_gain,
    key_gain,
    w_out,
    mixer_gain,
    expert_input,
    expert_ids,
    expert_weights,
    input_gain,
    w_gate,
    w_up,
    w_down,
    out_gain,
):
    n_ep = lax.axis_size("ep")
    n_x = w_gate.shape[0] * n_ep // GROUPS
    kv_heads = key_rows.shape[1] // query_gain.shape[0]
    if (
        kv_heads == GROUPS
        and GROUPS * n_x == n_ep
        and n_x == 2
        and expert_ids.shape[1] == n_x
        and w_gate.shape[0] == 1
        and lax.axis_size("tp") == 4
        and query_rows.shape[0] % GRID == 0
    ):
        return layer(
            n_x,
            query_rows,
            key_rows,
            value_rows,
            query_gain,
            key_gain,
            w_out,
            mixer_gain,
            expert_input,
            expert_ids,
            expert_weights,
            input_gain,
            w_gate,
            w_up,
            w_down,
            out_gain,
        )
    mixer_result = mixer_half(
        query_rows, key_rows, value_rows, query_gain, key_gain, w_out, mixer_gain
    )
    moe_result = expert_half(
        expert_input, expert_ids, expert_weights, input_gain, w_gate, w_up, w_down, out_gain
    )
    return (mixer_result, moe_result)


def solution(mesh):
    return jax.shard_map(
        per_device,
        mesh=mesh,
        in_specs=(
            P("ep", "tp"),
            P("ep", "tp"),
            P("ep", "tp"),
            P(),
            P(),
            P("tp", None),
            P(),
            P("ep", None),
            P("ep", None),
            P("ep", None),
            P(),
            P("ep", None, "tp"),
            P("ep", None, "tp"),
            P("ep", "tp", None),
            P("tp"),
        ),
        out_specs=(P(("ep", "tp"), None), P("ep", "tp")),
        check_vma=False,
    )
```
